256 devices in a mesh: ep: 16 (over y, x), tp: 16 (over z, core).
Axes of the slice: x: 4, y: 4, z: 8, core: 2. Of those that a mesh axis runs over, the one named last changes fastest.
Arguments:
- mix_query: bfloat16 [16384, 2048], P('ep', 'tp'), may hold values from -60 to 60
- mix_key: bfloat16 [16384, 2048], P('ep', 'tp'), may hold values from -60 to 60
- mix_value: bfloat16 [16384, 2048], P('ep', 'tp'), may hold values from -6 to 6
- head_lambda: float32 [16], P('tp'), may hold values from 0.3 to 0.8
- head_gain: float32 [128], replicated, may hold values from 0.1 to 1.9
- out_weight: bfloat16 [2048, 2048], P('tp'), may hold values from -0.125 to 0.125
- moe_input: bfloat16 [16384, 2048], P(('ep', 'tp')), may hold values from -6 to 6
- moe_gain: float32 [2048], replicated, may hold values from 0.1 to 1.9
- expert_ids: int32 [16384, 2], P(('ep', 'tp')), may hold values from 0 to 15, all different within a row; in each aligned block of 64 rows (0 to 63, 64 to 127, ...) at most 12 rows name the same one
- route_weight: float32 [16384, 2], P(('ep', 'tp')), may hold values from 0.2 to 1
- gate_weight: bfloat16 [16, 2048, 4096], P('ep', None, 'tp'), may hold values from -0.125 to 0.125
- up_weight: bfloat16 [16, 2048, 4096], P('ep', None, 'tp'), may hold values from -0.125 to 0.125
- down_weight: bfloat16 [16, 4096, 2048], P('ep', 'tp'), may hold values from -0.09375 to 0.09375
Outputs:
- mix_output: bfloat16 [16384, 2048], P(('ep', 'tp'))
- moe_output: bfloat16 [16384, 2048], P(('ep', 'tp'))
The draws below stay inside these ranges and needn't reach their ends.
Inputs may be any that keep to these rules, and one draw needn't show every extreme that they name: `expert_ids`: in each aligned block of 64 rows (the rows of one device) no expert is named by more than 12 rows; a row names 2 different experts.
All inputs are finite; a program needn't handle non-finite values.
Results may differ from the reference program's by a relative error of at most 0.02.
The reference program's roundings to bfloat16 on the way count: a program that leaves them out, or rounds other values in their place, can miss the bound.
Values may be sent and summed in bfloat16 or wider, within the bound.
A program may use at most 128 MiB of HBM per device.

```python
import math
import jax
import jax.numpy as jnp
import numpy as np
from jax import lax

D = 2048
HEADS = 16
HD = 64
FF = 4096
TOP = 2
ROWS_B = 64
VD = 128
HEADS_DEV = 1
FF_DEV = 256
EXPERTS = 16
CAP = 12
SEQ = 16384
TOKENS_B = 16384
N_TP = 16


def draw_query_side(key, stream):
    columns = HEADS * 2 * HD
    return jnp.clip(1.3 * jax.random.normal(jax.random.fold_in(key, stream), (SEQ, columns), jnp.float32), -8.0, 8.0)


def draw_mix_query(key, part):
    return draw_query_side(key, 11).astype(jnp.bfloat16)


def draw_mix_key(key, part):
    return draw_query_side(key, 13).astype(jnp.bfloat16)


def level_of(stream_key, extent, cuts, least, largest):
    factor_of, own = 1.0, jax.random.fold_in(stream_key, 6)
    for axis_at, parts in cuts:
        draws = jnp.exp(jax.random.uniform(jax.random.fold_in(own, axis_at), (parts,), jnp.float32, least / len(cuts), largest / len(cuts)))
        factor_of = factor_of * jnp.repeat(draws, extent[axis_at] // parts).reshape([-1 if axis == axis_at else 1 for axis in range(len(extent))])
    return factor_of


def assign_block(key, own, number, rows, number_of, top, most, lean):
    order = jax.random.permutation(key, number_of)
    packed, common = shares(number_of, rows * top, most, lean, True), shares(number_of, rows * top, most, lean, False)
    places = jnp.arange(number_of)

    def named(sizes, rotation):
        used = int((sizes > 0).sum())
        fixed = max(1, used // 4)
        passed = fixed + (places - fixed + rotation * (used - fixed)) % max(1, number_of - fixed)
        return jnp.zeros((number_of,), jnp.int32).at[order[jnp.where(places < fixed, places, passed)]].set(jnp.asarray(sizes, jnp.int32))

    sizes = jnp.where(number % 4 == 0, named(packed, number // 4), named(common, number - number // 4 - 1))
    mixed = jax.random.permutation(jax.random.fold_in(own, 3), number_of)
    source_of, receiver = mixed[0:number_of // 2 * 2:2], mixed[1:number_of // 2 * 2:2]
    room = jnp.minimum(sizes[source_of] - 1, most - sizes[receiver]) // 2
    room = jnp.where((source_of == order[0]) | (receiver == order[0]) | (sizes[receiver] == 0), 0, jnp.maximum(room, 0))
    passed = jax.random.randint(jax.random.fold_in(own, 4), (number_of // 2,), 0, 1 << 20) % (room + 1)
    sizes = sizes.at[source_of].add(-passed).at[receiver].add(passed)
    items = jnp.searchsorted(jnp.cumsum(sizes), jnp.arange(rows * top), side="right").astype(jnp.int32)
    grid = items.reshape(top, rows).T
    grid = grid[jax.random.permutation(jax.random.fold_in(own, 1), rows)]
    rotation = jax.random.randint(jax.random.fold_in(own, 2), (rows, 1), 0, top)
    return jnp.take_along_axis(grid, (jnp.arange(top)[None, :] + rotation) % top, axis=1)


def shares(count, total, reach, skew, full):
    weights = [(1 << 20) // math.isqrt(grade ** skew) + 1 for grade in range(1, count + 1)]
    largest = reach if full else min(reach, max(-(-total // count), total * weights[0] // sum(weights)))
    least = 1 if total - largest >= count - 1 else 0
    counts, rest = [largest] + [least] * (count - 1), total - largest - least * (count - 1)
    while rest > 0:
        candidates = [i for i in range(1, count) if counts[i] < largest] or [i for i in range(1, count) if counts[i] < reach]
        mass, budget = sum([weights[i] for i in candidates]), rest
        for i in candidates:
            addition = min(reach - counts[i], max(1, budget * weights[i] // mass), rest)
            counts[i] = counts[i] + addition
            rest = rest - addition
    return np.array(counts)


def scatter_about(stream_key, dims, scale, most, shards=(), held_as=jnp.bfloat16):
    gain = level_of(stream_key, dims, shards, -0.22, 0.18) if shards else 1.0
    drawn = jax.random.normal(stream_key, dims, jnp.float32) * scale * gain
    return jnp.minimum(jnp.maximum(drawn, -most), most).astype(held_as)


def setup_inputs(seed: int = 0) -> dict:
    splits = jax.random.split(jax.random.key(seed), 14)
    mix_query = draw_mix_query(jax.random.fold_in(splits[13], 71), 0)
    mix_key = draw_mix_key(jax.random.fold_in(splits[13], 71), 0)
    mix_value = scatter_about(splits[2], (SEQ, HEADS * VD), 1.0, 6.0, ((0, 16), (1, 16)))
    head_lambda = jnp.clip(0.3 + 0.5 * jax.random.uniform(splits[3], (HEADS,), jnp.float32) ** level_of(splits[3], (HEADS,), ((0, 16),), -0.2, 0.2), 0.3, 0.8)
    head_gain = jnp.clip(1.0 + 0.18 * jax.random.normal(splits[4], (VD,), jnp.float32), 0.1, 1.9)
    out_weight = scatter_about(splits[5], (HEADS * VD, D), (HEADS * VD) ** -0.5, 0.125, ((0, 16),))
    moe_input = scatter_about(splits[6], (TOKENS_B, D), 1.0, 6.0, ((0, 256),))
    moe_gain = jnp.clip(1.0 + 0.18 * jax.random.normal(splits[7], (D,), jnp.float32), 0.1, 1.9)
    expert_ids_keys = jax.random.split(jax.random.fold_in(splits[8], 1), TOKENS_B // ROWS_B)
    expert_ids_turns = jax.random.permutation(jax.random.fold_in(splits[8], 3), TOKENS_B // ROWS_B)
    expert_ids = jax.vmap(lambda own, number: assign_block(jax.random.fold_in(splits[8], 2), own, number, ROWS_B, EXPERTS, TOP, CAP, 2))(expert_ids_keys, expert_ids_turns).reshape((TOKENS_B, TOP))
    route_weight = jnp.clip(jnp.exp(math.log(1.0) - 1.609438 * jax.random.uniform(splits[9], (TOKENS_B, TOP), jnp.float32) ** level_of(splits[9], (TOKENS_B, TOP), ((0, 256),), -0.2, 0.2)), 0.2, 1.0)
    gate_weight = scatter_about(splits[10], (EXPERTS, D, FF), D ** -0.5, 0.125, ((0, 16), (2, 16)))
    up_weight = scatter_about(splits[11], (EXPERTS, D, FF), D ** -0.5, 0.125, ((0, 16), (2, 16)))
    down_weight = scatter_about(splits[12], (EXPERTS, FF, D), FF ** -0.5, 0.09375, ((0, 16), (1, 16)))
    return dict(mix_query=mix_query, mix_key=mix_key, mix_value=mix_value, head_lambda=head_lambda, head_gain=head_gain, out_weight=out_weight, moe_input=moe_input, moe_gain=moe_gain, expert_ids=expert_ids, route_weight=route_weight, gate_weight=gate_weight, up_weight=up_weight, down_weight=down_weight)


epsilon = 1e-06
rotary_base = 10000.0

def norm_rows(values, scales):
    square_mean = lax.optimization_barrier(jnp.mean(values * values, axis=-1, keepdims=True))
    return values * lax.rsqrt(square_mean + epsilon) * scales

def rotate(values, positions):
    half_dim = values.shape[-1] // 2
    frequency = rotary_base ** (-jnp.arange(half_dim, dtype=jnp.float32) * 2.0 / values.shape[-1])
    angles = positions.astype(jnp.float32)[:, None] * frequency[None, :]
    layout = (values.shape[0],) + (1,) * (values.ndim - 2) + (half_dim,)
    cosine = jnp.cos(angles).reshape(layout)
    sine_table = jnp.sin(angles).reshape(layout)
    leading = values[..., :half_dim]
    trailing = values[..., half_dim:]
    return jnp.concatenate([leading * cosine - trailing * sine_table, trailing * cosine + leading * sine_table], axis=-1)

def head_attention(members, head_gain):
    queries, keys, values, lambdas = members
    length = queries.shape[0]
    step_rows = math.gcd(length, 1024)
    blocks = length // step_rows

    def one_query_block(block_index):
        row_start = (block_index * step_rows).astype(jnp.int32)
        query_block = lax.dynamic_slice_in_dim(queries, row_start, step_rows, 0).astype(jnp.float32)
        query_pos = row_start + jnp.arange(step_rows, dtype=jnp.int32)

        def scores_of(key_index):
            key_start = (key_index * step_rows).astype(jnp.int32)
            key_block = lax.dynamic_slice_in_dim(keys, key_start, step_rows, 0).astype(jnp.float32)
            scores = jnp.einsum('qpd,kpd->pqk', query_block, key_block)
            key_pos = key_start + jnp.arange(step_rows, dtype=jnp.int32)
            visible = key_pos[None, :] <= query_pos[:, None]
            return (scores, visible[None, :, :], key_start)

        def find_max(key_index, running_max):
            scores, visible, unused = scores_of(key_index)
            return jnp.maximum(running_max, lax.optimization_barrier(jnp.max(jnp.where(visible, scores, -jnp.inf), axis=-1)))
        running_max = lax.fori_loop(0, block_index + 1, find_max, jnp.full((2, step_rows), -jnp.inf, jnp.float32))

        def accumulate(key_index, loop_state):
            totals, weighted = loop_state
            scores, visible, key_start = scores_of(key_index)
            expo = jnp.where(visible, jnp.exp(scores - running_max[:, :, None]), 0.0)
            rounded = lax.optimization_barrier(expo.astype(jnp.bfloat16)).astype(jnp.float32)
            value_block = lax.dynamic_slice_in_dim(values, key_start, step_rows, 0).astype(jnp.float32)
            return (totals + lax.optimization_barrier(jnp.sum(expo, axis=-1)), weighted + jnp.einsum('pqk,ke->pqe', rounded, value_block))
        initial = (jnp.zeros((2, step_rows), jnp.float32), jnp.zeros((2, step_rows, VD), jnp.float32))
        totals, weighted = lax.fori_loop(0, block_index + 1, accumulate, initial)
        combined_heads = weighted[0] / totals[0][:, None] - lambdas * weighted[1] / totals[1][:, None]
        return norm_rows(combined_heads, head_gain).astype(jnp.bfloat16)
    outputs = lax.map(one_query_block, jnp.arange(blocks, dtype=jnp.int32))
    return outputs.reshape(length, VD)

def mixer_half(mix_query, mix_key, mix_value, head_lambda, head_gain, out_weight):
    length = mix_query.shape[0]
    positions = jnp.arange(length, dtype=jnp.int32)
    queries = rotate(mix_query.astype(jnp.float32).reshape(length, HEADS, 2, HD), positions) * HD ** (-0.5)
    queries = lax.optimization_barrier(queries.astype(jnp.bfloat16))
    keys = rotate(mix_key.astype(jnp.float32).reshape(length, HEADS, 2, HD), positions)
    keys = lax.optimization_barrier(keys.astype(jnp.bfloat16))
    values = mix_value.reshape(length, HEADS, VD)

    def one_head(members):
        return head_attention(members, head_gain)
    heads_out = lax.map(one_head, (jnp.transpose(queries, (1, 0, 2, 3)), jnp.transpose(keys, (1, 0, 2, 3)), jnp.transpose(values, (1, 0, 2)), head_lambda))
    head_rows = jnp.transpose(heads_out, (1, 0, 2)).reshape(length, HEADS * VD)
    group_cols = HEADS_DEV * VD

    def add_group(group_index, totals):
        col_start = (group_index * group_cols).astype(jnp.int32)
        columns = lax.dynamic_slice_in_dim(head_rows, col_start, group_cols, 1)
        weight_rows = lax.dynamic_slice_in_dim(out_weight, col_start, group_cols, 0)
        partial_value = jnp.dot(columns, weight_rows, preferred_element_type=jnp.float32).astype(jnp.bfloat16)
        return totals + lax.optimization_barrier(partial_value).astype(jnp.float32)
    totals = lax.fori_loop(0, N_TP, add_group, jnp.zeros((length, D), jnp.float32))
    return totals.astype(jnp.bfloat16)

def experts_half(moe_input, moe_gain, expert_ids, route_weight, gate_weight, up_weight, down_weight):
    tokens = moe_input.shape[0]
    experts = gate_weight.shape[0]
    device_blocks = tokens // ROWS_B
    limit = device_blocks * CAP
    normed = norm_rows(moe_input.astype(jnp.float32), moe_gain).astype(jnp.bfloat16)
    normed = lax.optimization_barrier(normed)
    flat_ids = expert_ids.reshape(device_blocks, ROWS_B * TOP)
    member = (flat_ids[:, :, None] == jnp.arange(experts, dtype=jnp.int32)[None, None, :]).astype(jnp.int32)
    slot_rank = lax.optimization_barrier(jnp.sum(member * (jnp.cumsum(member, axis=1) - 1), axis=-1))
    destination = (jnp.arange(device_blocks, dtype=jnp.int32)[:, None] * CAP + slot_rank).reshape(tokens, TOP)

    def run_expert(expert_index, totals):
        routed = expert_ids == expert_index
        where_to = jnp.where(routed, destination, limit).astype(jnp.int32)
        buffer = jnp.zeros((limit, D), jnp.bfloat16)
        for choice_index in range(TOP):
            buffer = buffer.at[where_to[:, choice_index]].set(normed, mode='drop')
        gate_act = jnp.dot(buffer, gate_weight[expert_index], preferred_element_type=jnp.float32)
        upper = jnp.dot(buffer, up_weight[expert_index], preferred_element_type=jnp.float32)
        hidden = (jax.nn.silu(gate_act) * upper).astype(jnp.bfloat16)
        hidden = lax.optimization_barrier(hidden)
        down_here = down_weight[expert_index]

        def add_block(block_index, expert_out):
            col_start = (block_index * FF_DEV).astype(jnp.int32)
            columns = lax.dynamic_slice_in_dim(hidden, col_start, FF_DEV, 1)
            weight_rows = lax.dynamic_slice_in_dim(down_here, col_start, FF_DEV, 0)
            partial_value = jnp.dot(columns, weight_rows, preferred_element_type=jnp.float32).astype(jnp.bfloat16)
            return expert_out + lax.optimization_barrier(partial_value).astype(jnp.float32)
        expert_out = lax.fori_loop(0, N_TP, add_block, jnp.zeros((limit, D), jnp.float32)).astype(jnp.bfloat16)
        expert_out = lax.optimization_barrier(expert_out)
        for choice_index in range(TOP):
            picked = expert_out[jnp.minimum(where_to[:, choice_index], limit - 1)].astype(jnp.float32)
            contribution = route_weight[:, choice_index][:, None] * picked
            totals = totals + jnp.where(routed[:, choice_index][:, None], contribution, 0.0)
        return totals
    totals = lax.fori_loop(0, experts, run_expert, jnp.zeros((tokens, D), jnp.float32))
    return totals.astype(jnp.bfloat16)

def reference(mix_query, mix_key, mix_value, head_lambda, head_gain, out_weight, moe_input, moe_gain, expert_ids, route_weight, gate_weight, up_weight, down_weight):
    mix_output = mixer_half(mix_query, mix_key, mix_value, head_lambda, head_gain, out_weight)
    moe_output = experts_half(moe_input, moe_gain, expert_ids, route_weight, gate_weight, up_weight, down_weight)
    return (mix_output, moe_output)
```

```python
import functools

import jax
import jax.numpy as jnp
from jax import lax
from jax.experimental import pallas as pl
from jax.experimental.pallas import tpu as pltpu
from jax.sharding import PartitionSpec as P

epsilon = 1e-06
rotary_base = 10000.0
far_below = -1e30
MESH = pl.DeviceIdType.MESH
F32 = jnp.float32
BF16 = jnp.bfloat16
PAD = 16


def remote(src, dst, send, recv, ep, tp):
    return pltpu.make_async_remote_copy(
        src_ref=src, dst_ref=dst, send_sem=send, recv_sem=recv,
        device_id={"ep": ep, "tp": tp}, device_id_type=MESH,
    )


def kernel(cfg, *refs):
    (NE, NZ, SL, DM, FFD, ROWS, CAP) = cfg
    (q_hbm, k_hbm, v_hbm, lam_ref, gain_ref, wo_hbm, x_hbm, mgain_ref, ids_ref, rw_ref,
     wg_hbm, wu_hbm, wd_hbm, cos_ref, sin_ref,
     mix_ref, moe_ref,
     xin, q_in, k_in, v_in, wg, wu, wd, wo, disp, A, X, Y, RU, RD, RET, B,
     KA, VT, Q2, acc, m_s, l_s, hb, hx, MY, MRU, MRD,
     in_sem, wsend, wrecv, dsend, drecv, kvsend, kvrecv,
     agus, agur, agds, agdr, rsus, rsur, rsds, rsdr, rtsend, rtrecv, hsend, hrecv,
     mus, mur, mds, mdr) = refs

    E = lax.axis_index("ep")
    T = lax.axis_index("tp")
    Z = T // 2
    C = T % 2
    up_t = 2 * ((Z + 1) % NZ) + C
    dn_t = 2 * ((Z + NZ - 1) % NZ) + C
    par_t = 2 * Z + (1 - C)
    SLOTS = NE * CAP
    HALF = SLOTS // 2
    HEADS_W = 128
    PS = NE * PAD

    def local(src, dst, i):
        return pltpu.make_async_copy(src, dst, in_sem.at[i])

    c_x = local(x_hbm, xin, 0)
    c_k = local(k_hbm, k_in, 1)
    c_v = local(v_hbm, v_in, 2)
    c_q = local(q_hbm, q_in, 3)
    c_w = [local(wg_hbm.at[0], wg.at[0], 4), local(wu_hbm.at[0], wu.at[0], 5),
           local(wd_hbm.at[0], wd.at[0], 6), local(wo_hbm, wo.at[0], 7)]
    for c in (c_x, c_k, c_v, c_q, *c_w):
        c.start()

    barrier = pltpu.get_barrier_semaphore()

    def greet(j, _):
        pl.semaphore_signal(barrier, inc=1, device_id={"ep": (E + j) % NE, "tp": T}, device_id_type=MESH)
        return 0

    lax.fori_loop(1, NE, greet, 0)
    for t in (up_t, dn_t, par_t):
        pl.semaphore_signal(barrier, inc=1, device_id={"ep": E, "tp": t}, device_id_type=MESH)

    ids = ids_ref[...]
    lane = lax.broadcasted_iota(jnp.int32, (ROWS, 128), 1)
    hot = [(ids[:, j:j + 1] == lane).astype(F32) for j in range(2)]
    r_i = lax.broadcasted_iota(jnp.int32, (ROWS, ROWS), 0)
    c_i = lax.broadcasted_iota(jnp.int32, (ROWS, ROWS), 1)
    below = (c_i < r_i).astype(BF16)
    before = jnp.dot(below, (hot[0] + hot[1]).astype(BF16), preferred_element_type=F32)
    slot_lane = lax.broadcasted_iota(jnp.int32, (ROWS, PS), 1)
    sel = []
    for j in range(2):
        rank = jnp.sum(hot[j] * before, axis=1, keepdims=True).astype(jnp.int32)
        slot = ids[:, j:j + 1] * PAD + rank
        sel.append((slot == slot_lane).astype(BF16))

    c_x.wait()
    xv = xin[...].astype(F32)
    normed = (xv * lax.rsqrt(jnp.mean(xv * xv, axis=-1, keepdims=True) + epsilon) * mgain_ref[...]).astype(BF16)
    both = sel[0] + sel[1]
    for n in range(0, DM, 512):
        nn = min(512, DM)
        disp[:, n:n + nn] = lax.dot_general(
            both, normed[:, n:n + nn], (((0,), (0,)), ((), ())), preferred_element_type=F32
        ).astype(BF16)

    pl.semaphore_wait(barrier, NE - 1 + 3)

    def rows_of(buf, e):
        return buf.at[pl.ds(pl.multiple_of(e * PAD, PAD), PAD)]

    def disp_copy(j):
        dst = (E + j) % NE
        return remote(rows_of(disp, dst), rows_of(A, E), dsend.at[j], drecv.at[E], dst, T)

    def send_disp(j, _):
        disp_copy(j).start()
        return 0

    lax.fori_loop(1, NE, send_disp, 0)
    own = pl.ds(pl.multiple_of(E * PAD, PAD), PAD)
    A[own, :] = disp[own, :]

    w_copies = [
        remote(wg_hbm.at[0], wg.at[1], wsend.at[0], wrecv.at[0], E, par_t),
        remote(wu_hbm.at[0], wu.at[1], wsend.at[1], wrecv.at[1], E, par_t),
        remote(wd_hbm.at[0], wd.at[1], wsend.at[2], wrecv.at[2], E, par_t),
        remote(wo_hbm, wo.at[1], wsend.at[3], wrecv.at[3], E, par_t),
    ]
    for c in w_copies:
        c.start()

    cosv, sinv = cos_ref[...], sin_ref[...]

    def rotated(xt):
        parts = []
        for m in range(2):
            a = xt[64 * m:64 * m + 32, :]
            b = xt[64 * m + 32:64 * m + 64, :]
            parts.append(a * cosv - b * sinv)
            parts.append(b * cosv + a * sinv)
        return jnp.concatenate(parts, axis=0)

    c_k.wait()
    kt = rotated(k_in[...].astype(F32).T)
    KA[E] = kt.T.astype(BF16)
    c_v.wait()
    VT[E] = v_in[...].T

    def kv_copies(j):
        dst = (E + j) % NE
        return (remote(KA.at[E], KA.at[E], kvsend.at[0, j], kvrecv.at[0, E], dst, T),
                remote(VT.at[E], VT.at[E], kvsend.at[1, j], kvrecv.at[1, E], dst, T))

    def send_kv(j, _):
        @pl.when(E + j < NE)
        def _():
            for c in kv_copies(j):
                c.start()
        return 0

    lax.fori_loop(1, NE, send_kv, 0)

    c_q.wait()
    qt = (rotated(q_in[...].astype(F32).T) * 64 ** (-0.5)).astype(BF16)
    zero = jnp.zeros((64, SL), BF16)
    Q2[:, :SL] = jnp.concatenate([qt[:64], zero], axis=0)
    Q2[:, SL:] = jnp.concatenate([zero, qt[64:]], axis=0)
    acc[...] = jnp.zeros(acc.shape, F32)
    m_s[...] = jnp.full(m_s.shape, far_below, F32)
    l_s[...] = jnp.zeros(l_s.shape, F32)

    QT = min(512, SL)

    def attend(s, c0, keys, masked):
        cols = pl.ds(pl.multiple_of(c0, QT), QT)
        sc = jnp.dot(KA[s, :keys], Q2[:, cols], preferred_element_type=F32)
        if masked is not None:
            kk = lax.broadcasted_iota(jnp.int32, sc.shape, 0)
            qq = lax.broadcasted_iota(jnp.int32, sc.shape, 1) + masked
            sc = jnp.where(kk <= qq, sc, far_below)
        m_old = m_s[:, cols]
        m_new = jnp.maximum(m_old, jnp.max(sc, axis=0, keepdims=True))
        p = jnp.exp(sc - m_new)
        shrink = jnp.exp(m_old - m_new)
        m_s[:, cols] = m_new
        l_s[:, cols] = l_s[:, cols] * shrink + jnp.sum(p, axis=0, keepdims=True)
        acc[:, cols] = acc[:, cols] * shrink + jnp.dot(
            VT[s, :, :keys], p.astype(BF16), preferred_element_type=F32)

    def diag(mp, _):
        for q0 in range(0, SL, QT):
            attend(E, mp * SL + q0, q0 + QT, q0)
        return 0

    lax.fori_loop(0, 2, diag, 0)

    def kv_block(j):
        src = E - 1 - j

        @pl.when(j < E)
        def _():
            remote(KA.at[src], KA.at[src], kvsend.at[0, 0], kvrecv.at[0, src], E, T).wait_recv()
            remote(VT.at[src], VT.at[src], kvsend.at[1, 0], kvrecv.at[1, src], E, T).wait_recv()

            def tile(t, _):
                attend(src, t * QT, SL, None)
                return 0

            lax.fori_loop(0, 2 * SL // QT, tile, 0)

    def half_rows(h):
        return pl.ds(pl.multiple_of(h * HALF, HALF), HALF)

    def ag_up(zs, h, j):
        ref = X.at[zs, half_rows(h)]
        return remote(ref, ref, agus.at[j], agur.at[j], E, up_t)

    def ag_dn(zs, h, j):
        ref = X.at[zs, half_rows(h)]
        return remote(ref, ref, agds.at[j], agdr.at[j], E, dn_t)

    c_row = lax.broadcasted_iota(jnp.int32, (HALF, PS // 2), 0)
    c_col = lax.broadcasted_iota(jnp.int32, (HALF, PS // 2), 1)
    pack = jnp.zeros((HALF, PS // 2), jnp.bool_)
    for g in range(NE // 2):
        pack = pack | ((c_row >= g * CAP) & (c_row < (g + 1) * CAP) & (c_col == c_row + g * (PAD - CAP)))
    pack = pack.astype(BF16)

    for h in range(2):
        def wait_rows(s, _):
            @pl.when(s != E)
            def _():
                remote(rows_of(disp, s), rows_of(A, s), dsend.at[0], drecv.at[s], E, T).wait_recv()
            return 0

        lax.fori_loop(h * (NE // 2), (h + 1) * (NE // 2), wait_rows, 0)
        for n in range(0, DM, 512):
            nn = min(512, DM)
            X[Z, h * HALF:(h + 1) * HALF, n:n + nn] = jnp.dot(
                pack, A[h * PS // 2:(h + 1) * PS // 2, n:n + nn], preferred_element_type=F32).astype(BF16)
        if h == 0:
            ag_up(Z, 0, 0).start()
            if NZ > 2:
                ag_dn(Z, 0, 1).start()
        else:
            ag_dn(Z, 1, 0).start()
            if NZ > 2:
                ag_up(Z, 1, 1).start()

    for c in c_w:
        c.wait()
    for c in w_copies:
        c.wait_recv()

    def experts(zb):
        xb = X[zb]
        hid = []
        for w in range(2):
            g = jnp.dot(xb, wg[w], preferred_element_type=F32)
            u = jnp.dot(xb, wu[w], preferred_element_type=F32)
            hid.append((g / (1.0 + jnp.exp(-g)) * u).astype(BF16))
        for n in range(0, DM, 512):
            nn = min(512, DM)
            y = jnp.dot(hid[0], wd[0, :, n:n + nn], preferred_element_type=F32)
            y += jnp.dot(hid[1], wd[1, :, n:n + nn], preferred_element_type=F32)
            Y[zb, :, n:n + nn] = y.astype(BF16)

    def ring_parts(buf, land_u, land_d, rows, us, ur, ds_, dr):
        def place(h):
            return pl.ds(pl.multiple_of(h * rows, rows), rows)

        def up(j):
            d = (Z + NZ // 2 - (j + 1) // 2 + NZ) % NZ
            h = (j + 1) % 2
            return d, place(h), remote(buf.at[d, place(h)], land_u.at[j], us.at[j], ur.at[j], E, up_t)

        def down(j):
            d = (Z - NZ // 2 + (j + 1) // 2 + NZ) % NZ
            h = j % 2
            return d, place(h), remote(buf.at[d, place(h)], land_d.at[j], ds_.at[j], dr.at[j], E, dn_t)

        def first(j):
            up(j)[2].start()
            down(j)[2].start()

        def step(j):
            for f, land in ((up, land_u), (down, land_d)):
                f(j - 2)[2].wait_recv()
                d, where, copy = f(j)
                buf[d, where, :] = (buf[d, where, :].astype(F32) + land[j - 2].astype(F32)).astype(BF16)
                copy.start()

        def last(out):
            for j in ((NZ - 3, NZ - 2) if NZ > 2 else (0,)):
                up(j)[2].wait_recv()
                down(j)[2].wait_recv()
            for h in range(2):
                if NZ > 2:
                    ju, jd = (NZ - 3, NZ - 2) if h == 0 else (NZ - 2, NZ - 3)
                    s = buf[Z, h * rows:(h + 1) * rows, :].astype(F32) + land_u[ju].astype(F32) + land_d[jd].astype(F32)
                else:
                    s = buf[Z, h * rows:(h + 1) * rows, :].astype(F32) + (land_d[0] if h == 0 else land_u[0]).astype(F32)
                out(h, s.astype(BF16))

        def drain(j, _):
            up(j)[2].wait_send()
            down(j)[2].wait_send()
            return 0

        return first, step, last, drain

    y_first, y_step, y_last, y_drain = ring_parts(Y, RU, RD, HALF, rsus, rsur, rsds, rsdr)
    MR = ROWS // 2
    m_first, m_step, m_last, m_drain = ring_parts(MY, MRU, MRD, MR, mus, mur, mds, mdr)

    STEPS = (NZ - 1) + max(NZ - 2, 1)
    NKV = NE - 1

    def main(i, _):
        @pl.when(i < NZ - 1)
        def _():
            k = i // 2 + 1
            h = i % 2
            zu = (Z - k + NZ) % NZ
            zd = (Z + k) % NZ
            ag_up(zu, h, i).wait_recv()
            if NZ > 2:
                @pl.when(i < NZ - 3)
                def _():
                    ag_up(zu, h, i + 2).start()
            ag_dn(zd, 1 - h, i).wait_recv()
            if NZ > 2:
                @pl.when(i < NZ - 3)
                def _():
                    ag_dn(zd, 1 - h, i + 2).start()

        @pl.when(i < NZ)
        def _():
            k = (i + 1) // 2
            zb = (Z + k * (1 - 2 * (i % 2)) + NZ) % NZ
            experts(zb)

        @pl.when(i == NZ - 1)
        def _():
            y_first(0)
            if NZ > 2:
                y_first(1)

        if NZ > 2:
            @pl.when(i >= NZ)
            def _():
                y_step(i - NZ + 2)

        def blocks(j, _):
            kv_block(j)
            return 0

        lax.fori_loop((i * NKV) // STEPS, ((i + 1) * NKV) // STEPS, blocks, 0)
        return 0

    lax.fori_loop(0, STEPS, main, 0)

    o = acc[...] / l_s[...]
    comb = o[:, :SL] - lam_ref[0] * o[:, SL:]
    comb = comb * lax.rsqrt(jnp.mean(comb * comb, axis=0, keepdims=True) + epsilon)
    heads = (comb.T * gain_ref[...]).astype(BF16)
    for t in range(2 * NZ):
        hb[t % 2, (t // 2) * ROWS:(t // 2 + 1) * ROWS, :] = heads[t * ROWS:(t + 1) * ROWS, :]
    h_copy = remote(hb.at[1 - C], hx, hsend.at[0], hrecv.at[0], E, par_t)
    h_copy.start()

    u_row = lax.broadcasted_iota(jnp.int32, (PS // 2, HALF), 0)
    u_col = lax.broadcasted_iota(jnp.int32, (PS // 2, HALF), 1)
    unpack = jnp.zeros((PS // 2, HALF), jnp.bool_)
    for g in range(NE // 2):
        unpack = unpack | ((u_col >= g * CAP) & (u_col < (g + 1) * CAP) & (u_row == u_col + g * (PAD - CAP)))
    unpack = unpack.astype(BF16)

    def spread(h, s):
        for n in range(0, DM, 512):
            nn = min(512, DM)
            RET[h * PS // 2:(h + 1) * PS // 2, n:n + nn] = jnp.dot(
                unpack, s[:, n:n + nn], preferred_element_type=F32).astype(BF16)

    y_last(spread)

    def ret_copy(j):
        dst = (E + j) % NE
        return remote(rows_of(RET, dst), rows_of(B, E), rtsend.at[j], rtrecv.at[E], dst, T)

    def send_ret(j, _):
        ret_copy(j).start()
        return 0

    lax.fori_loop(1, NE, send_ret, 0)
    B[own, :] = RET[own, :]

    h_copy.wait_recv()
    for zd in range(NZ):
        ha = hb[C, zd * ROWS:(zd + 1) * ROWS, :]
        hc = hx[zd * ROWS:(zd + 1) * ROWS, :]
        for n in range(0, DM, 512):
            nn = min(512, DM)
            MY[zd, :, n:n + nn] = (jnp.dot(ha, wo[0, :, n:n + nn], preferred_element_type=F32)
                                   + jnp.dot(hc, wo[1, :, n:n + nn], preferred_element_type=F32)).astype(BF16)
    m_first(0)
    if NZ > 2:
        m_first(1)

    def wait_ret(s, _):
        @pl.when(s != E)
        def _():
            remote(rows_of(RET, s), rows_of(B, s), rtsend.at[0], rtrecv.at[s], E, T).wait_recv()
        return 0

    if NZ > 2:
        def m_loop(j, _):
            m_step(j)
            return 0

        lax.fori_loop(2, NZ - 1, m_loop, 0)

    lax.fori_loop(0, NE, wait_ret, 0)
    rw = rw_ref[...]
    for n in range(0, DM, 512):
        nn = min(512, DM)
        bb = B[:, n:n + nn]
        moe_ref[:, n:n + nn] = (
            rw[:, 0:1] * jnp.dot(sel[0], bb, preferred_element_type=F32)
            + rw[:, 1:2] * jnp.dot(sel[1], bb, preferred_element_type=F32)).astype(BF16)

    def mix_out(h, s):
        mix_ref[h * MR:(h + 1) * MR, :] = s

    m_last(mix_out)

    def drain_ep(j, _):
        disp_copy(j).wait_send()
        ret_copy(j).wait_send()

        @pl.when(E + j < NE)
        def _():
            for c in kv_copies(j):
                c.wait_send()
        return 0

    lax.fori_loop(1, NE, drain_ep, 0)
    for c in (*w_copies, h_copy):
        c.wait_send()

    def drain_z(j, _):
        ag_up(Z, 0, j).wait_send()
        ag_dn(Z, 0, j).wait_send()
        y_drain(j, 0)
        m_drain(j, 0)
        return 0

    lax.fori_loop(0, NZ - 1, drain_z, 0)


def make_body(cap):
    def body(mix_query, mix_key, mix_value, head_lambda, head_gain, out_weight, moe_input, moe_gain,
             expert_ids, route_weight, gate_weight, up_weight, down_weight):
        NE = lax.axis_size("ep")
        NZ = lax.axis_size("tp") // 2
        SL = mix_query.shape[0]
        ROWS, DM = moe_input.shape
        FFD = gate_weight.shape[2]
        CAP = cap if cap else 3 * ROWS * expert_ids.shape[1] // (2 * NE)
        pos = (lax.axis_index("ep") * SL + jnp.arange(SL, dtype=jnp.int32)).astype(F32)
        freq = rotary_base ** (-jnp.arange(32, dtype=F32) * 2.0 / 64)
        ang = freq[:, None] * pos[None, :]
        cosv, sinv = jnp.cos(ang), jnp.sin(ang)
        cfg = (NE, NZ, SL, DM, FFD, ROWS, CAP)
        SLOTS, PS = NE * CAP, NE * PAD
        HALF = SLOTS // 2
        N1 = NZ - 1
        VM, DMA = pltpu.VMEM, pltpu.SemaphoreType.DMA
        any_ = pl.BlockSpec(memory_space=pl.ANY)
        vm = pl.BlockSpec(memory_space=pltpu.VMEM)
        sm = pl.BlockSpec(memory_space=pltpu.SMEM)
        scratch = [
            VM((ROWS, DM), BF16), VM((SL, 128), BF16), VM((SL, 128), BF16), VM((SL, 128), BF16),
            VM((2, DM, FFD), BF16), VM((2, DM, FFD), BF16), VM((2, FFD, DM), BF16), VM((2, 128, DM), BF16),
            VM((PS, DM), BF16), VM((PS, DM), BF16),
            VM((NZ, SLOTS, DM), BF16), VM((NZ, SLOTS, DM), BF16),
            VM((N1, HALF, DM), BF16), VM((N1, HALF, DM), BF16),
            VM((PS, DM), BF16), VM((PS, DM), BF16),
            VM((NE, SL, 128), BF16), VM((NE, 128, SL), BF16), VM((128, 2 * SL), BF16),
            VM((128, 2 * SL), F32), VM((1, 2 * SL), F32), VM((1, 2 * SL), F32),
            VM((2, SL // 2, 128), BF16), VM((SL // 2, 128), BF16),
            VM((NZ, ROWS, DM), BF16), VM((N1, ROWS // 2, DM), BF16), VM((N1, ROWS // 2, DM), BF16),
            DMA((8,)), DMA((4,)), DMA((4,)), DMA((NE,)), DMA((NE,)), DMA((2, NE)), DMA((2, NE)),
            DMA((N1,)), DMA((N1,)), DMA((N1,)), DMA((N1,)),
            DMA((N1,)), DMA((N1,)), DMA((N1,)), DMA((N1,)),
            DMA((NE,)), DMA((NE,)), DMA((1,)), DMA((1,)),
            DMA((N1,)), DMA((N1,)), DMA((N1,)), DMA((N1,)),
        ]
        return pl.pallas_call(
            functools.partial(kernel, cfg),
            out_shape=(jax.ShapeDtypeStruct((ROWS, DM), BF16), jax.ShapeDtypeStruct((ROWS, DM), BF16)),
            in_specs=[any_, any_, any_, sm, vm, any_, any_, vm, vm, vm, any_, any_, any_, vm, vm],
            out_specs=(vm, vm),
            scratch_shapes=scratch,
            compiler_params=pltpu.CompilerParams(
                collective_id=0, has_side_effects=True, vmem_limit_bytes=67043328),
            name="step",
        )(mix_query, mix_key, mix_value, head_lambda, head_gain.reshape(1, -1), out_weight, moe_input,
          moe_gain.reshape(1, -1), expert_ids, route_weight, gate_weight, up_weight, down_weight, cosv, sinv)

    return body


def solution(mesh, cap=None):
    return jax.shard_map(
        make_body(cap),
        mesh=mesh,
        in_specs=(
            P("ep", "tp"), P("ep", "tp"), P("ep", "tp"), P("tp"), P(), P("tp", None),
            P(("ep", "tp"), None), P(), P(("ep", "tp"), None), P(("ep", "tp"), None),
            P("ep", None, "tp"), P("ep", None, "tp"), P("ep", "tp", None),
        ),
        out_specs=(P(("ep", "tp"), None), P(("ep", "tp"), None)),
        check_vma=False,
    )
```

```python
import functools
import math

import jax
import jax.numpy as jnp
from jax import lax
from jax.experimental import pallas as pl
from jax.experimental.pallas import tpu as pltpu
from jax.sharding import PartitionSpec as P

epsilon = 1e-06
rotary_base = 10000.0
far_below = -1e30
MESH = pl.DeviceIdType.MESH
scope = jax.named_scope
F32 = jnp.float32
BF16 = jnp.bfloat16
PAD = 16


def remote(src, dst, send, recv, ep, tp):
    return pltpu.make_async_remote_copy(
        src_ref=src, dst_ref=dst, send_sem=send, recv_sem=recv,
        device_id={"ep": ep, "tp": tp}, device_id_type=MESH,
    )


def kernel(cfg, *refs):
    (NE, NZ, SL, DM, FFD, ROWS, CAP) = cfg
    (q_hbm, k_hbm, v_hbm, lam_ref, gain_ref, wo_hbm, x_hbm, mgain_ref, ids_ref, rw_ref,
     wg_hbm, wu_hbm, wd_hbm, cos_ref, sin_ref,
     mix_ref, moe_ref,
     xin, q_in, k_in, v_in, wg, wu, wd, wo, disp, A, X, Y, RU, RD, RET, B,
     KA, VT, Q2, acc, m_s, l_s, hb, hx, MY, MRU, MRD,
     in_sem, wsend, wrecv, dsend, drecv, kvsend, kvrecv,
     agus, agur, agds, agdr, rsus, rsur, rsds, rsdr, rtsend, rtrecv, hsend, hrecv,
     mus, mur, mds, mdr) = refs

    E = lax.axis_index("ep")
    T = lax.axis_index("tp")
    Z = T // 2
    C = T % 2
    up_t = 2 * ((Z + 1) % NZ) + C
    dn_t = 2 * ((Z + NZ - 1) % NZ) + C
    par_t = 2 * Z + (1 - C)
    NX = math.isqrt(NE)
    NY = NE // NX
    x_at, y_at = E % NX, E // NX
    SLOTS = NE * CAP
    HALF = SLOTS // 2
    HEADS_W = 128
    PS = NE * PAD

    def local(src, dst, i):
        return pltpu.make_async_copy(src, dst, in_sem.at[i])

    c_x = local(x_hbm, xin, 0)
    c_k = local(k_hbm, k_in, 1)
    c_v = local(v_hbm, v_in, 2)
    c_q = local(q_hbm, q_in, 3)
    c_w = [local(wg_hbm.at[0], wg.at[0], 4), local(wu_hbm.at[0], wu.at[0], 5),
           local(wd_hbm.at[0], wd.at[0], 6), local(wo_hbm, wo.at[0], 7)]
    for c in (c_x, c_k, c_v, c_q, *c_w):
        c.start()

    barrier = pltpu.get_barrier_semaphore()

    def greet(j, _):
        pl.semaphore_signal(barrier, inc=1, device_id={"ep": (E + j) % NE, "tp": T}, device_id_type=MESH)
        return 0

    lax.fori_loop(1, NE, greet, 0)
    for t in (up_t, dn_t, par_t):
        pl.semaphore_signal(barrier, inc=1, device_id={"ep": E, "tp": t}, device_id_type=MESH)

    ids = ids_ref[...]
    lane = lax.broadcasted_iota(jnp.int32, (ROWS, 128), 1)
    hot = [(ids[:, j:j + 1] == lane).astype(F32) for j in range(2)]
    r_i = lax.broadcasted_iota(jnp.int32, (ROWS, ROWS), 0)
    c_i = lax.broadcasted_iota(jnp.int32, (ROWS, ROWS), 1)
    below = (c_i < r_i).astype(BF16)
    before = jnp.dot(below, (hot[0] + hot[1]).astype(BF16), preferred_element_type=F32)
    slot_lane = lax.broadcasted_iota(jnp.int32, (ROWS, PS), 1)
    sel = []
    for j in range(2):
        rank = jnp.sum(hot[j] * before, axis=1, keepdims=True).astype(jnp.int32)
        slot = ids[:, j:j + 1] * PAD + rank
        sel.append((slot == slot_lane).astype(BF16))

    with scope("xwait"):
        c_x.wait()
    xv = xin[...].astype(F32)
    normed = (xv * lax.rsqrt(jnp.mean(xv * xv, axis=-1, keepdims=True) + epsilon) * mgain_ref[...]).astype(BF16)
    both = sel[0] + sel[1]
    for n in range(0, DM, 512):
        nn = min(512, DM)
        disp[:, n:n + nn] = lax.dot_general(
            both, normed[:, n:n + nn], (((0,), (0,)), ((), ())), preferred_element_type=F32
        ).astype(BF16)

    with scope("barrier"):
        pl.semaphore_wait(barrier, NE - 1 + 3)

    def rows_of(buf, e):
        return buf.at[pl.ds(pl.multiple_of(e * PAD, PAD), PAD)]

    def disp_copy(j):
        dst = (E + j) % NE
        return remote(rows_of(disp, dst), rows_of(A, E), dsend.at[j], drecv.at[E], dst, T)

    def send_disp(j, _):
        disp_copy(j).start()
        return 0

    lax.fori_loop(1, NE, send_disp, 0)
    own = pl.ds(pl.multiple_of(E * PAD, PAD), PAD)
    A[own, :] = disp[own, :]

    w_copies = [
        remote(wg_hbm.at[0], wg.at[1], wsend.at[0], wrecv.at[0], E, par_t),
        remote(wu_hbm.at[0], wu.at[1], wsend.at[1], wrecv.at[1], E, par_t),
        remote(wd_hbm.at[0], wd.at[1], wsend.at[2], wrecv.at[2], E, par_t),
        remote(wo_hbm, wo.at[1], wsend.at[3], wrecv.at[3], E, par_t),
    ]
    for c in w_copies:
        c.start()

    cosv, sinv = cos_ref[...], sin_ref[...]

    def rotated(xt):
        parts = []
        for m in range(2):
            a = xt[64 * m:64 * m + 32, :]
            b = xt[64 * m + 32:64 * m + 64, :]
            parts.append(a * cosv - b * sinv)
            parts.append(b * cosv + a * sinv)
        return jnp.concatenate(parts, axis=0)

    with scope("kprep"):
        c_k.wait()
        kt = rotated(k_in[...].astype(F32).T)
        KA[E] = kt.T.astype(BF16)
        c_v.wait()
        VT[E] = v_in[...].T

    def pass_key(s, send, x2, y2):
        return remote(KA.at[s], KA.at[s], kvsend.at[0, send], kvrecv.at[0, s], y2 * NX + x2, T)

    def pass_value(s, send, x2, y2):
        return remote(VT.at[s], VT.at[s], kvsend.at[1, send], kvrecv.at[1, s], y2 * NX + x2, T)

    def key_down(act):
        for y2 in range(NY):
            @pl.when(y2 > y_at)
            def _():
                act(pass_key(E, NE + y2, x_at, y2))

    def key_along(ys, act):
        for x2 in range(NX):
            @pl.when((x2 != x_at) & ((ys < y_at) | (x2 > x_at)))
            def _():
                act(pass_key(ys * NX + x_at, ys * NX + x2, x2, y_at))

    def value_along(act):
        for x2 in range(NX):
            @pl.when((x2 != x_at) & ((y_at < NY - 1) | (x2 > x_at)))
            def _():
                act(pass_value(E, NE + x2, x2, y_at))

    def value_down(xs, act):
        for y2 in range(NY):
            @pl.when(y2 > y_at)
            def _():
                act(pass_value(y_at * NX + xs, y2 * NX + xs, x_at, y2))

    def start(c):
        c.start()

    def sent(c):
        c.wait_send()

    FWD = max(NX, NY) - 1

    def pass_on(f):
        ys = y_at - 1 - f

        @pl.when(ys >= 0)
        def _():
            with scope("kfwait"):
                pass_key(ys * NX + x_at, 0, x_at, y_at).wait_recv()
            key_along(ys, start)

        xs = (x_at + 1 + f) % NX

        @pl.when((f < NX - 1) & ((y_at < NY - 1) | (xs < x_at)))
        def _():
            with scope("vfwait"):
                pass_value(y_at * NX + xs, 0, x_at, y_at).wait_recv()
            value_down(xs, start)

    c_q.wait()
    qt = (rotated(q_in[...].astype(F32).T) * 64 ** (-0.5)).astype(BF16)
    zero = jnp.zeros((64, SL), BF16)
    Q2[:, :SL] = jnp.concatenate([qt[:64], zero], axis=0)
    Q2[:, SL:] = jnp.concatenate([zero, qt[64:]], axis=0)
    acc[...] = jnp.zeros(acc.shape, F32)
    m_s[...] = jnp.full(m_s.shape, far_below, F32)
    l_s[...] = jnp.zeros(l_s.shape, F32)

    QT = min(512, SL)

    def attend(s, c0, keys, masked):
        cols = pl.ds(pl.multiple_of(c0, QT), QT)
        sc = jnp.dot(KA[s, :keys], Q2[:, cols], preferred_element_type=F32)
        if masked is not None:
            kk = lax.broadcasted_iota(jnp.int32, sc.shape, 0)
            qq = lax.broadcasted_iota(jnp.int32, sc.shape, 1) + masked
            sc = jnp.where(kk <= qq, sc, far_below)
        m_old = m_s[:, cols]
        m_new = jnp.maximum(m_old, jnp.max(sc, axis=0, keepdims=True))
        p = jnp.exp(sc - m_new)
        shrink = jnp.exp(m_old - m_new)
        m_s[:, cols] = m_new
        l_s[:, cols] = l_s[:, cols] * shrink + jnp.sum(p, axis=0, keepdims=True)
        acc[:, cols] = acc[:, cols] * shrink + jnp.dot(
            VT[s, :, :keys], p.astype(BF16), preferred_element_type=F32)

    def diag(mp, _):
        for q0 in range(0, SL, QT):
            attend(E, mp * SL + q0, q0 + QT, q0)
        return 0

    with scope("diag"):
        lax.fori_loop(0, 2, diag, 0)

    def kv_block(j):
        src = E - 1 - j

        @pl.when(j < E)
        def _():
            with scope("kvwait"):
                @pl.when(src % NX != x_at)
                def _():
                    pass_key(src, 0, x_at, y_at).wait_recv()

                @pl.when(src // NX != y_at)
                def _():
                    pass_value(src, 0, x_at, y_at).wait_recv()

            def tile(t, _):
                attend(src, t * QT, SL, None)
                return 0

            with scope("attend"):
                lax.fori_loop(0, 2 * SL // QT, tile, 0)

    def half_rows(h):
        return pl.ds(pl.multiple_of(h * HALF, HALF), HALF)

    def ag_up(zs, h, j):
        ref = X.at[zs, half_rows(h)]
        return remote(ref, ref, agus.at[j], agur.at[j], E, up_t)

    def ag_dn(zs, h, j):
        ref = X.at[zs, half_rows(h)]
        return remote(ref, ref, agds.at[j], agdr.at[j], E, dn_t)

    c_row = lax.broadcasted_iota(jnp.int32, (HALF, PS // 2), 0)
    c_col = lax.broadcasted_iota(jnp.int32, (HALF, PS // 2), 1)
    pack = jnp.zeros((HALF, PS // 2), jnp.bool_)
    for g in range(NE // 2):
        pack = pack | ((c_row >= g * CAP) & (c_row < (g + 1) * CAP) & (c_col == c_row + g * (PAD - CAP)))
    pack = pack.astype(BF16)

    for h in range(2):
        def wait_rows(s, _):
            @pl.when(s != E)
            def _():
                remote(rows_of(disp, s), rows_of(A, s), dsend.at[0], drecv.at[s], E, T).wait_recv()
            return 0

        with scope("rowswait"):
            lax.fori_loop(h * (NE // 2), (h + 1) * (NE // 2), wait_rows, 0)
        for n in range(0, DM, 512):
            nn = min(512, DM)
            X[Z, h * HALF:(h + 1) * HALF, n:n + nn] = jnp.dot(
                pack, A[h * PS // 2:(h + 1) * PS // 2, n:n + nn], preferred_element_type=F32).astype(BF16)
        if h == 0:
            ag_up(Z, 0, 0).start()
            if NZ > 2:
                ag_dn(Z, 0, 1).start()
        else:
            ag_dn(Z, 1, 0).start()
            if NZ > 2:
                ag_up(Z, 1, 1).start()

    key_down(start)
    value_along(start)
    key_along(y_at, start)
    value_down(x_at, start)

    with scope("wwait"):
        for c in c_w:
            c.wait()
        for c in w_copies:
            c.wait_recv()

    def experts(zb):
        xb = X[zb]
        hid = []
        for w in range(2):
            g = jnp.dot(xb, wg[w], preferred_element_type=F32)
            u = jnp.dot(xb, wu[w], preferred_element_type=F32)
            hid.append((g / (1.0 + jnp.exp(-g)) * u).astype(BF16))
        for n in range(0, DM, 512):
            nn = min(512, DM)
            y = jnp.dot(hid[0], wd[0, :, n:n + nn], preferred_element_type=F32)
            y += jnp.dot(hid[1], wd[1, :, n:n + nn], preferred_element_type=F32)
            Y[zb, :, n:n + nn] = y.astype(BF16)

    def ring_parts(buf, land_u, land_d, rows, us, ur, ds_, dr):
        def place(h):
            return pl.ds(pl.multiple_of(h * rows, rows), rows)

        def up(j):
            d = (Z + NZ // 2 - (j + 1) // 2 + NZ) % NZ
            h = (j + 1) % 2
            return d, place(h), remote(buf.at[d, place(h)], land_u.at[j], us.at[j], ur.at[j], E, up_t)

        def down(j):
            d = (Z - NZ // 2 + (j + 1) // 2 + NZ) % NZ
            h = j % 2
            return d, place(h), remote(buf.at[d, place(h)], land_d.at[j], ds_.at[j], dr.at[j], E, dn_t)

        def first(j):
            up(j)[2].start()
            down(j)[2].start()

        def step(j):
            for f, land in ((up, land_u), (down, land_d)):
                with scope("rswait"):
                    f(j - 2)[2].wait_recv()
                d, where, copy = f(j)
                with scope("rsadd"):
                    buf[d, where, :] = (buf[d, where, :].astype(F32) + land[j - 2].astype(F32)).astype(BF16)
                copy.start()

        def last(out):
            for j in ((NZ - 3, NZ - 2) if NZ > 2 else (0,)):
                with scope("lastwait"):
                    up(j)[2].wait_recv()
                    down(j)[2].wait_recv()
            for h in range(2):
                if NZ > 2:
                    ju, jd = (NZ - 3, NZ - 2) if h == 0 else (NZ - 2, NZ - 3)
                    s = buf[Z, h * rows:(h + 1) * rows, :].astype(F32) + land_u[ju].astype(F32) + land_d[jd].astype(F32)
                else:
                    s = buf[Z, h * rows:(h + 1) * rows, :].astype(F32) + (land_d[0] if h == 0 else land_u[0]).astype(F32)
                out(h, s.astype(BF16))

        def drain(j, _):
            up(j)[2].wait_send()
            down(j)[2].wait_send()
            return 0

        return first, step, last, drain

    y_first, y_step, y_last, y_drain = ring_parts(Y, RU, RD, HALF, rsus, rsur, rsds, rsdr)
    MR = ROWS // 2
    m_first, m_step, m_last, m_drain = ring_parts(MY, MRU, MRD, MR, mus, mur, mds, mdr)

    STEPS = (NZ - 1) + max(NZ - 2, 1)
    NKV = NE - 1

    def block_at(i):
        return jnp.maximum(jnp.minimum(i, NZ) - FWD, 0) + 2 * jnp.maximum(i - NZ, 0)

    def main(i, _):
        @pl.when(i < NZ - 1)
        def _():
            k = i // 2 + 1
            h = i % 2
            zu = (Z - k + NZ) % NZ
            zd = (Z + k) % NZ
            with scope("agwait"):
                ag_up(zu, h, i).wait_recv()
            if NZ > 2:
                @pl.when(i < NZ - 3)
                def _():
                    ag_up(zu, h, i + 2).start()
            with scope("agwait2"):
                ag_dn(zd, 1 - h, i).wait_recv()
            if NZ > 2:
                @pl.when(i < NZ - 3)
                def _():
                    ag_dn(zd, 1 - h, i + 2).start()

        @pl.when(i < NZ)
        def _():
            k = (i + 1) // 2
            zb = (Z + k * (1 - 2 * (i % 2)) + NZ) % NZ
            with scope("experts"):
                experts(zb)

        @pl.when(i == NZ - 1)
        def _():
            y_first(0)
            if NZ > 2:
                y_first(1)

        if NZ > 2:
            @pl.when(i >= NZ)
            def _():
                y_step(i - NZ + 2)

        @pl.when(i < FWD)
        def _():
            pass_on(i)

        def blocks(j, _):
            kv_block(j)
            return 0

        lax.fori_loop(block_at(i), jnp.where(i == STEPS - 1, NKV, block_at(i + 1)), blocks, 0)
        return 0

    lax.fori_loop(0, STEPS, main, 0)

    with scope("endloop"):
        pass
    o = acc[...] / l_s[...]
    comb = o[:, :SL] - lam_ref[0] * o[:, SL:]
    comb = comb * lax.rsqrt(jnp.mean(comb * comb, axis=0, keepdims=True) + epsilon)
    heads = (comb.T * gain_ref[...]).astype(BF16)
    for t in range(2 * NZ):
        hb[t % 2, (t // 2) * ROWS:(t // 2 + 1) * ROWS, :] = heads[t * ROWS:(t + 1) * ROWS, :]
    h_copy = remote(hb.at[1 - C], hx, hsend.at[0], hrecv.at[0], E, par_t)
    h_copy.start()

    u_row = lax.broadcasted_iota(jnp.int32, (PS // 2, HALF), 0)
    u_col = lax.broadcasted_iota(jnp.int32, (PS // 2, HALF), 1)
    unpack = jnp.zeros((PS // 2, HALF), jnp.bool_)
    for g in range(NE // 2):
        unpack = unpack | ((u_col >= g * CAP) & (u_col < (g + 1) * CAP) & (u_row == u_col + g * (PAD - CAP)))
    unpack = unpack.astype(BF16)

    def spread(h, s):
        for n in range(0, DM, 512):
            nn = min(512, DM)
            RET[h * PS // 2:(h + 1) * PS // 2, n:n + nn] = jnp.dot(
                unpack, s[:, n:n + nn], preferred_element_type=F32).astype(BF16)

    y_last(spread)

    def ret_copy(j):
        dst = (E + j) % NE
        return remote(rows_of(RET, dst), rows_of(B, E), rtsend.at[j], rtrecv.at[E], dst, T)

    def send_ret(j, _):
        ret_copy(j).start()
        return 0

    lax.fori_loop(1, NE, send_ret, 0)
    B[own, :] = RET[own, :]

    with scope("hwait"):
        h_copy.wait_recv()
    for zd in range(NZ):
        ha = hb[C, zd * ROWS:(zd + 1) * ROWS, :]
        hc = hx[zd * ROWS:(zd + 1) * ROWS, :]
        for n in range(0, DM, 512):
            nn = min(512, DM)
            MY[zd, :, n:n + nn] = (jnp.dot(ha, wo[0, :, n:n + nn], preferred_element_type=F32)
                                   + jnp.dot(hc, wo[1, :, n:n + nn], preferred_element_type=F32)).astype(BF16)
    with scope("mfirst"):
        m_first(0)
    if NZ > 2:
        m_first(1)

    def wait_ret(s, _):
        @pl.when(s != E)
        def _():
            remote(rows_of(RET, s), rows_of(B, s), rtsend.at[0], rtrecv.at[s], E, T).wait_recv()
        return 0

    if NZ > 2:
        def m_loop(j, _):
            m_step(j)
            return 0

        lax.fori_loop(2, NZ - 1, m_loop, 0)

    with scope("retwait"):
        lax.fori_loop(0, NE, wait_ret, 0)
    rw = rw_ref[...]
    for n in range(0, DM, 512):
        nn = min(512, DM)
        bb = B[:, n:n + nn]
        moe_ref[:, n:n + nn] = (
            rw[:, 0:1] * jnp.dot(sel[0], bb, preferred_element_type=F32)
            + rw[:, 1:2] * jnp.dot(sel[1], bb, preferred_element_type=F32)).astype(BF16)

    def mix_out(h, s):
        mix_ref[h * MR:(h + 1) * MR, :] = s

    m_last(mix_out)

    def drain_ep(j, _):
        disp_copy(j).wait_send()
        ret_copy(j).wait_send()
        return 0

    with scope("drain"):
        lax.fori_loop(1, NE, drain_ep, 0)
    for c in (*w_copies, h_copy):
        c.wait_send()
    key_down(sent)
    value_along(sent)
    for ys in range(NY):
        @pl.when(ys <= y_at)
        def _():
            key_along(ys, sent)
    for xs in range(NX):
        value_down(xs, sent)

    def drain_z(j, _):
        ag_up(Z, 0, j).wait_send()
        ag_dn(Z, 0, j).wait_send()
        y_drain(j, 0)
        m_drain(j, 0)
        return 0

    lax.fori_loop(0, NZ - 1, drain_z, 0)


def make_body(cap):
    def body(mix_query, mix_key, mix_value, head_lambda, head_gain, out_weight, moe_input, moe_gain,
             expert_ids, route_weight, gate_weight, up_weight, down_weight):
        NE = lax.axis_size("ep")
        NZ = lax.axis_size("tp") // 2
        SL = mix_query.shape[0]
        ROWS, DM = moe_input.shape
        FFD = gate_weight.shape[2]
        CAP = cap if cap else 3 * ROWS * expert_ids.shape[1] // (2 * NE)
        pos = (lax.axis_index("ep") * SL + jnp.arange(SL, dtype=jnp.int32)).astype(F32)
        freq = rotary_base ** (-jnp.arange(32, dtype=F32) * 2.0 / 64)
        ang = freq[:, None] * pos[None, :]
        cosv, sinv = jnp.cos(ang), jnp.sin(ang)
        cfg = (NE, NZ, SL, DM, FFD, ROWS, CAP)
        SLOTS, PS = NE * CAP, NE * PAD
        HALF = SLOTS // 2
        N1 = NZ - 1
        VM, DMA = pltpu.VMEM, pltpu.SemaphoreType.DMA
        any_ = pl.BlockSpec(memory_space=pl.ANY)
        vm = pl.BlockSpec(memory_space=pltpu.VMEM)
        sm = pl.BlockSpec(memory_space=pltpu.SMEM)
        scratch = [
            VM((ROWS, DM), BF16), VM((SL, 128), BF16), VM((SL, 128), BF16), VM((SL, 128), BF16),
            VM((2, DM, FFD), BF16), VM((2, DM, FFD), BF16), VM((2, FFD, DM), BF16), VM((2, 128, DM), BF16),
            VM((PS, DM), BF16), VM((PS, DM), BF16),
            VM((NZ, SLOTS, DM), BF16), VM((NZ, SLOTS, DM), BF16),
            VM((N1, HALF, DM), BF16), VM((N1, HALF, DM), BF16),
            VM((PS, DM), BF16), VM((PS, DM), BF16),
            VM((NE, SL, 128), BF16), VM((NE, 128, SL), BF16), VM((128, 2 * SL), BF16),
            VM((128, 2 * SL), F32), VM((1, 2 * SL), F32), VM((1, 2 * SL), F32),
            VM((2, SL // 2, 128), BF16), VM((SL // 2, 128), BF16),
            VM((NZ, ROWS, DM), BF16), VM((N1, ROWS // 2, DM), BF16), VM((N1, ROWS // 2, DM), BF16),
            DMA((8,)), DMA((4,)), DMA((4,)), DMA((NE,)), DMA((NE,)), DMA((2, 2 * NE)), DMA((2, NE)),
            DMA((N1,)), DMA((N1,)), DMA((N1,)), DMA((N1,)),
            DMA((N1,)), DMA((N1,)), DMA((N1,)), DMA((N1,)),
            DMA((NE,)), DMA((NE,)), DMA((1,)), DMA((1,)),
            DMA((N1,)), DMA((N1,)), DMA((N1,)), DMA((N1,)),
        ]
        return pl.pallas_call(
            functools.partial(kernel, cfg),
            out_shape=(jax.ShapeDtypeStruct((ROWS, DM), BF16), jax.ShapeDtypeStruct((ROWS, DM), BF16)),
            in_specs=[any_, any_, any_, sm, vm, any_, any_, vm, vm, vm, any_, any_, any_, vm, vm],
            out_specs=(vm, vm),
            scratch_shapes=scratch,
            compiler_params=pltpu.CompilerParams(
                collective_id=0, has_side_effects=True, vmem_limit_bytes=67043328),
            name="step",
        )(mix_query, mix_key, mix_value, head_lambda, head_gain.reshape(1, -1), out_weight, moe_input,
          moe_gain.reshape(1, -1), expert_ids, route_weight, gate_weight, up_weight, down_weight, cosv, sinv)

    return body


def solution(mesh, cap=None):
    return jax.shard_map(
        make_body(cap),
        mesh=mesh,
        in_specs=(
            P("ep", "tp"), P("ep", "tp"), P("ep", "tp"), P("tp"), P(), P("tp", None),
            P(("ep", "tp"), None), P(), P(("ep", "tp"), None), P(("ep", "tp"), None),
            P("ep", None, "tp"), P("ep", None, "tp"), P("ep", "tp", None),
        ),
        out_specs=(P(("ep", "tp"), None), P(("ep", "tp"), None)),
        check_vma=False,
    )
```

```python
import functools
import math

import jax
import jax.numpy as jnp
from jax import lax
from jax.experimental import pallas as pl
from jax.experimental.pallas import tpu as pltpu
from jax.sharding import PartitionSpec as P

epsilon = 1e-06
rotary_base = 10000.0
far_below = -1e30
MESH = pl.DeviceIdType.MESH
F32 = jnp.float32
BF16 = jnp.bfloat16
scope = jax.named_scope
NQ = 4


def remote(src, dst, send, recv, ep, tp):
    return pltpu.make_async_remote_copy(
        src_ref=src, dst_ref=dst, send_sem=send, recv_sem=recv,
        device_id={"ep": ep, "tp": tp}, device_id_type=MESH,
    )


def start(c):
    c.start()


def sent(c):
    c.wait_send()


def dot(a, b):
    return jnp.dot(a, b, preferred_element_type=F32)


def iota(shape, dim):
    return lax.broadcasted_iota(jnp.int32, shape, dim)


def one(x):
    return x.astype(F32).astype(BF16)


def kernel(cfg, *refs):
    (NE, NZ, SL, DM, FFD, ROWS, CAP) = cfg
    (q_hbm, k_hbm, v_hbm, lam_ref, gain_ref, wo_hbm, x_hbm, mgain_ref, ids_ref, rw_ref,
     wg_hbm, wu_hbm, wd_hbm, freq_ref,
     mix_ref, moe_ref,
     xin, q_in, k_in, v_in, wg, wu, wd, wo, disp, A, X, Y, RU, RD, RET, B, pack, unpack,
     KA, VT, Q2, acc, m_s, l_s, S0, S1, hb, hx, MY, MRU, MRD,
     in_sem, wsend, wrecv, dsend, drecv, kvsend, kvrecv,
     agus, agur, agds, agdr, rsus, rsur, rsds, rsdr, rtsend, rtrecv, hsend, hrecv,
     mus, mur, mds, mdr) = refs

    E = lax.axis_index("ep")
    T = lax.axis_index("tp")
    Z = T // 2
    C = T % 2
    up_t = 2 * ((Z + 1) % NZ) + C
    dn_t = 2 * ((Z + NZ - 1) % NZ) + C
    par_t = 2 * Z + (1 - C)
    NX = math.isqrt(NE)
    NY = NE // NX
    x_at, y_at = E % NX, E // NX
    SLOTS = NE * CAP
    G = 4
    FC = G * CAP
    FR = NE * FC
    QC = DM // NQ
    GW = QC // G
    H2 = NZ // 2

    def local(src, dst, i):
        return pltpu.make_async_copy(src, dst, in_sem.at[i])

    c_x = local(x_hbm, xin, 0)
    c_k = local(k_hbm, k_in, 1)
    c_v = local(v_hbm, v_in, 2)
    c_q = local(q_hbm, q_in, 3)
    c_w = [local(wg_hbm.at[0], wg.at[0], 4), local(wu_hbm.at[0], wu.at[0], 5),
           local(wd_hbm.at[0], wd.at[0], 6), local(wo_hbm, wo.at[0], 7)]
    for c in (c_x, c_k, c_v, c_q, *c_w):
        c.start()

    barrier = pltpu.get_barrier_semaphore()

    def greet(j, _):
        pl.semaphore_signal(barrier, inc=1, device_id={"ep": (E + j) % NE, "tp": T}, device_id_type=MESH)
        return 0

    lax.fori_loop(1, NE, greet, 0)
    for t in (up_t, dn_t, par_t):
        pl.semaphore_signal(barrier, inc=1, device_id={"ep": E, "tp": t}, device_id_type=MESH)

    ids = ids_ref[...]
    hot = [(ids[j:j + 1, :] == iota((NE, ROWS), 0)).astype(F32) for j in range(2)]
    earlier = one(iota((ROWS, ROWS), 0) < iota((ROWS, ROWS), 1))
    before = dot((hot[0] + hot[1]).astype(BF16), earlier)
    slot = []
    for j in range(2):
        rank = jnp.sum(hot[j] * before, axis=0, keepdims=True).astype(jnp.int32)
        slot.append(ids[j:j + 1, :] * FC + rank)
    folded = [jnp.concatenate([s + g * CAP for g in range(G)], axis=1) for s in slot]
    fr = iota((FR, G * ROWS), 0)
    send_sel = one((fr == folded[0]) | (fr == folded[1]))

    with scope("xwait"):
        c_x.wait()
    xv = xin[...].astype(F32)
    normed = (xv * lax.rsqrt(jnp.mean(xv * xv, axis=-1, keepdims=True) + epsilon) * mgain_ref[...]).astype(BF16)
    for q in range(NQ):
        part = jnp.concatenate([normed[:, q * QC + g * GW:q * QC + (g + 1) * GW] for g in range(G)], axis=0)
        disp[:, q * GW:(q + 1) * GW] = dot(send_sel, part).astype(BF16)

    def fold_of(i):
        f = i.astype(F32)
        g = jnp.floor((f + 0.5) * (1.0 / SLOTS))
        t = f - g * SLOTS
        return (t + jnp.floor((t + 0.5) * (1.0 / CAP)) * (FC - CAP) + g * CAP).astype(jnp.int32)

    pack[...] = one(fold_of(iota((G * SLOTS, 1), 0)) == iota((G * SLOTS, FR), 1))
    unpack[...] = one(fold_of(iota((1, G * SLOTS), 1)) == iota((FR, G * SLOTS), 0))

    eye32 = (iota((32, 32), 0) == iota((32, 32), 1)).astype(F32)
    freq = jnp.sum(eye32 * freq_ref[...], axis=1, keepdims=True)
    pos = (iota((32, SL), 1) + E * SL).astype(F32)
    ang = freq * pos
    cosv, sinv = jnp.cos(ang), jnp.sin(ang)

    with scope("barrier"):
        pl.semaphore_wait(barrier, NE - 1 + 3)

    def rows_of(buf, e, q):
        return buf.at[pl.ds(pl.multiple_of(e * FC, FC), FC), pl.ds(q * GW, GW)]

    def others(buf, q):
        return buf.at[pl.ds(0, (NE - 1) * FC), pl.ds(q * GW, GW)]

    for q in range(NQ):
        def send_disp(j, _):
            dst = (E + j) % NE
            remote(rows_of(disp, dst, q), rows_of(A, E, q), dsend.at[q], drecv.at[q], dst, T).start()
            return 0

        lax.fori_loop(1, NE, send_disp, 0)
    own = pl.ds(pl.multiple_of(E * FC, FC), FC)
    A[own, :] = disp[own, :]

    w_copies = [
        remote(wg_hbm.at[0], wg.at[1], wsend.at[0], wrecv.at[0], E, par_t),
        remote(wu_hbm.at[0], wu.at[1], wsend.at[1], wrecv.at[1], E, par_t),
        remote(wd_hbm.at[0], wd.at[1], wsend.at[2], wrecv.at[2], E, par_t),
        remote(wo_hbm, wo.at[1], wsend.at[3], wrecv.at[3], E, par_t),
    ]
    for c in w_copies:
        c.start()

    def rotated(xt):
        parts = []
        for m in range(2):
            a = xt[64 * m:64 * m + 32, :]
            b = xt[64 * m + 32:64 * m + 64, :]
            parts.append(a * cosv - b * sinv)
            parts.append(b * cosv + a * sinv)
        return jnp.concatenate(parts, axis=0)

    with scope("kprep"):
        c_k.wait()
        kt = rotated(k_in[...].astype(F32).T)
        KA[E] = kt.T.astype(BF16)
        c_v.wait()
        VT[E] = v_in[...].T

    def pass_key(s, send, x2, y2):
        return remote(KA.at[s], KA.at[s], kvsend.at[0, send], kvrecv.at[0, s], y2 * NX + x2, T)

    def pass_value(s, send, x2, y2):
        return remote(VT.at[s], VT.at[s], kvsend.at[1, send], kvrecv.at[1, s], y2 * NX + x2, T)

    def key_down(act):
        for y2 in range(NY):
            @pl.when(y2 > y_at)
            def _():
                act(pass_key(E, NE + y2, x_at, y2))

    def key_along(ys, act):
        for x2 in range(NX):
            @pl.when((x2 != x_at) & ((ys < y_at) | (x2 > x_at)))
            def _():
                act(pass_key(ys * NX + x_at, ys * NX + x2, x2, y_at))

    def value_along(act):
        for x2 in range(NX):
            @pl.when((x2 != x_at) & ((y_at < NY - 1) | (x2 > x_at)))
            def _():
                act(pass_value(E, NE + x2, x2, y_at))

    def value_down(xs, act):
        for y2 in range(NY):
            @pl.when(y2 > y_at)
            def _():
                act(pass_value(y_at * NX + xs, y2 * NX + xs, x_at, y2))

    FWD = max(NX, NY) - 1
    P1 = NX + NY - 2

    def pass_on(f):
        ys = y_at - 1 - f

        @pl.when(ys >= 0)
        def _():
            with scope("kfwait"):
                pass_key(ys * NX + x_at, 0, x_at, y_at).wait_recv()
            key_along(ys, start)

        xs = (x_at - 1 - f + NX) % NX

        @pl.when((f < NX - 1) & ((y_at < NY - 1) | (xs < x_at)))
        def _():
            with scope("vfwait"):
                pass_value(y_at * NX + xs, 0, x_at, y_at).wait_recv()
            value_down(xs, start)

    c_q.wait()
    qt = (rotated(q_in[...].astype(F32).T) * 64 ** (-0.5)).astype(BF16)
    zero = jnp.zeros((64, SL), BF16)
    Q2[:, :SL] = jnp.concatenate([qt[:64], zero], axis=0)
    Q2[:, SL:] = jnp.concatenate([zero, qt[64:]], axis=0)
    acc[...] = jnp.zeros(acc.shape, F32)
    m_s[...] = jnp.full(m_s.shape, far_below, F32)
    l_s[...] = jnp.zeros(l_s.shape, F32)

    QT = min(512, SL)

    def diag(mp, _):
        for q0 in range(0, SL, QT):
            keys = q0 + QT
            cols = pl.ds(pl.multiple_of(mp * SL + q0, QT), QT)
            sc = dot(KA[E, :keys], Q2[:, cols])
            sc = jnp.where(iota(sc.shape, 0) <= iota(sc.shape, 1) + q0, sc, far_below)
            m_new = jnp.max(sc, axis=0, keepdims=True)
            p = jnp.exp(sc - m_new)
            m_s[:, cols] = m_new
            l_s[:, cols] = jnp.sum(p, axis=0, keepdims=True)
            acc[:, cols] = dot(VT[E, :, :keys], p.astype(BF16))
        return 0

    with scope("diag"):
        lax.fori_loop(0, 2, diag, 0)

    SB = (S0, S1)
    TILES = 2 * SL // QT

    def attend(s):
        def scores(t):
            sc = dot(KA[s], Q2[:, t * QT:(t + 1) * QT])
            SB[t % 2][...] = sc
            return jnp.max(sc, axis=0, keepdims=True)

        top = scores(0)
        for t in range(TILES):
            cols = slice(t * QT, (t + 1) * QT)
            m_old = m_s[:, cols]
            m_new = jnp.maximum(m_old, top)
            shrink = jnp.exp(m_old - m_new)
            m_s[:, cols] = m_new
            if t + 1 < TILES:
                top = scores(t + 1)
            p = jnp.exp(SB[t % 2][...] - m_new)
            l_s[:, cols] = l_s[:, cols] * shrink + jnp.sum(p, axis=0, keepdims=True)
            acc[:, cols] = acc[:, cols] * shrink + dot(VT[s], p.astype(BF16))

    def kv_block(j):
        r = j - P1
        rest = (y_at - 1 - r // max(NX - 1, 1)) * NX + (x_at + 1 + r % max(NX - 1, 1)) % NX
        near = jnp.where(j < x_at, E - 1 - j, E - (j - x_at + 1) * NX)
        src = jnp.where(r < 0, near, rest)

        @pl.when(((r < 0) & (j < x_at + y_at)) | ((r >= 0) & (r < y_at * (NX - 1))))
        def _():
            with scope("kvwait"):
                @pl.when(src % NX != x_at)
                def _():
                    pass_key(src, 0, x_at, y_at).wait_recv()

                @pl.when(src // NX != y_at)
                def _():
                    pass_value(src, 0, x_at, y_at).wait_recv()

            with scope("attend"):
                attend(src)

    def ag_up(zs, q, i):
        ref = X.at[zs, q]
        return remote(ref, ref, agus.at[i], agur.at[i], E, up_t)

    def ag_dn(zs, q, i):
        ref = X.at[zs, q]
        return remote(ref, ref, agds.at[i], agdr.at[i], E, dn_t)

    for q in range(NQ):
        with scope("rowswait"):
            remote(others(disp, q), others(A, q), dsend.at[q], drecv.at[q], E, T).wait_recv()
        rows = dot(pack[...], A[:, q * GW:(q + 1) * GW])
        for g in range(G):
            X[Z, q, :, g * GW:(g + 1) * GW] = rows[g * SLOTS:(g + 1) * SLOTS].astype(BF16)
        if NZ > 2 or q < 2:
            ag_up(Z, q, q).start()
        if NZ > 2 or q >= 2:
            ag_dn(Z, q, q if NZ > 2 else q - 2).start()

    key_down(start)
    value_along(start)
    key_along(y_at, start)
    value_down(x_at, start)

    with scope("wwait"):
        for c in c_w:
            c.wait()
        for c in w_copies:
            c.wait_recv()

    def experts(zb):
        xb = jnp.concatenate([X[zb, q] for q in range(NQ)], axis=1)
        hid = []
        for w in range(2):
            g = dot(xb, wg[w])
            u = dot(xb, wu[w])
            hid.append((g / (1.0 + jnp.exp(-g)) * u).astype(BF16))
        for q in range(NQ):
            n = slice(q * QC, (q + 1) * QC)
            Y[zb, q] = (dot(hid[0], wd[0, :, n]) + dot(hid[1], wd[1, :, n])).astype(BF16)

    def make_ring(buf, land_u, land_d, us, ur, ds_, dr):
        def target(t, sign):
            return (Z + sign * (H2 - (t + 1) // 2) + NZ) % NZ

        def up(t, i):
            far = 1 - jnp.minimum(t, 1)
            h = (t + 1) % 2 - far
            ref = buf.at[target(t, 1), 2 * h + i]
            return ref, remote(ref, land_u.at[2 * t + i], us.at[2 * t + i], ur.at[2 * t + i], E, up_t)

        def down(t, i):
            h = (t + 1) % 2
            ref = buf.at[target(t, -1), 2 * h + i]
            return ref, remote(ref, land_d.at[2 * t + i], ds_.at[2 * t + i], dr.at[2 * t + i], E, dn_t)

        def first():
            for i in range(2):
                up(0, i)[1].start()
                down(0, i)[1].start()
            if NZ > 2:
                for i in range(2):
                    up(2, i)[1].start()
                    down(1, i)[1].start()

        def step(s):
            for f, land, t in ((up, land_u, s + 1 - (2 - jnp.minimum(s, 2))), (down, land_d, s + 1)):
                for i in range(2):
                    with scope("rswait"):
                        f(s - 1, i)[1].wait_recv()
                    ref, copy = f(t, i)
                    ref[...] = (ref[...].astype(F32) + land[2 * (s - 1) + i].astype(F32)).astype(BF16)
                    copy.start()

        def last(out):
            if NZ > 2:
                for h in range(2):
                    t = NZ - 3 + h
                    for i in range(2):
                        with scope("lastwait"):
                            up(t, i)[1].wait_recv()
                            down(t, i)[1].wait_recv()
                        q = 2 * h + i
                        out(q, (buf[Z, q].astype(F32) + land_u[2 * t + i].astype(F32)
                                + land_d[2 * t + i].astype(F32)).astype(BF16))
            else:
                for q in range(NQ):
                    f, land = (up, land_u) if q < 2 else (down, land_d)
                    f(0, q % 2)[1].wait_recv()
                    out(q, (buf[Z, q].astype(F32) + land[q % 2].astype(F32)).astype(BF16))

        def drain(t, _):
            for i in range(2):
                up(t, i)[1].wait_send()
                down(t, i)[1].wait_send()
            return 0

        return first, step, last, drain

    y_first, y_step, y_last, y_drain = make_ring(Y, RU, RD, rsus, rsur, rsds, rsdr)
    m_first, m_step, m_last, m_drain = make_ring(MY, MRU, MRD, mus, mur, mds, mdr)

    AGS = NZ - 1
    FWD0 = max(min(2, AGS - FWD), 0)
    STEPS = AGS + max(NZ - 3, 0)
    NKV = NE - 1
    counts = {12: [0, 0, 1, 1, 2, 1, 1, 2, 2, 2, 2, 1]}.get(STEPS)
    if counts is None or NE != 16:
        counts = [0] * (STEPS - 1) + [NKV]

    def after(i, n):
        return jnp.clip(i - n + 1, 0, 1)

    def block_at(i):
        return sum(c * after(i, s + 1) for s, c in enumerate(counts) if c)

    def main(i, _):
        @pl.when(i < AGS)
        def _():
            k = i // 2 + 1
            h = i % 2
            zu = (Z - k + NZ) % NZ
            zd = (Z + k) % NZ
            final = after(i, AGS - 1)
            for n in range(2):
                with scope("agwait"):
                    ag_up(zu, 2 * h + n, 2 * i + n).wait_recv()
                if NZ > 2:
                    @pl.when(i < NZ - 3)
                    def _():
                        ag_up(zu, 2 * h + n, 2 * i + n + 4).start()
            hd = h + final
            for n in range(2):
                with scope("agwait2"):
                    ag_dn(zd, 2 * hd + n, 2 * i + n).wait_recv()
                if NZ > 2:
                    @pl.when((i < NZ - 4) | (i == NZ - 3))
                    def _():
                        ag_dn(zd, 2 * hd + n, 2 * i + n + 4 - 2 * after(i, NZ - 3)).start()

            @pl.when((i >= FWD0) & (i < FWD0 + FWD))
            def _():
                pass_on(i - FWD0)

            def block(b, _):
                kb = (b + 1) // 2
                with scope("experts"):
                    experts((Z + kb * (1 - 2 * (b % 2)) + NZ) % NZ)
                return 0

            lo = i + (after(i, NZ - 2) if NZ > 2 else 0)
            lax.fori_loop(lo, i + 1 + (after(i, NZ - 3) if NZ > 2 else 1), block, 0)

        @pl.when(i == AGS - 1)
        def _():
            y_first()

        if NZ > 2:
            @pl.when(i >= AGS)
            def _():
                y_step(i - AGS + 1)

        def blocks(j, _):
            kv_block(j)
            return 0

        lax.fori_loop(block_at(i), block_at(i + 1), blocks, 0)
        return 0

    lax.fori_loop(0, STEPS, main, 0)

    with scope("endloop"):
        o = acc[...] / l_s[...]
    comb = o[:, :SL] - lam_ref[0] * o[:, SL:]
    comb = comb * lax.rsqrt(jnp.mean(comb * comb, axis=0, keepdims=True) + epsilon)
    heads = (comb.T * gain_ref[...]).astype(BF16)
    for t in range(2 * NZ):
        hb[t % 2, (t // 2) * ROWS:(t // 2 + 1) * ROWS, :] = heads[t * ROWS:(t + 1) * ROWS, :]
    h_copy = remote(hb.at[1 - C], hx, hsend.at[0], hrecv.at[0], E, par_t)
    h_copy.start()

    with scope("hwait"):
        h_copy.wait_recv()
    for q in range(NQ):
        n = slice(q * QC, (q + 1) * QC)
        part = (dot(hb[C], wo[0, :, n]) + dot(hx[...], wo[1, :, n])).astype(BF16)
        for zd in range(NZ):
            MY[zd, q] = part[zd * ROWS:(zd + 1) * ROWS]
    with scope("mfirst"):
        m_first()
    def give_back(q, s):
        part = jnp.concatenate([s[:, g * GW:(g + 1) * GW] for g in range(G)], axis=0)
        RET[:, q * GW:(q + 1) * GW] = dot(unpack[...], part).astype(BF16)

        def send_ret(j, _):
            dst = (E + j) % NE
            remote(rows_of(RET, dst, q), rows_of(B, E, q), rtsend.at[q], rtrecv.at[q], dst, T).start()
            return 0

        lax.fori_loop(1, NE, send_ret, 0)

    y_last(give_back)
    B[own, :] = RET[own, :]

    if NZ > 2:
        def m_loop(s, _):
            m_step(s)
            return 0

        lax.fori_loop(1, NZ - 2, m_loop, 0)

    eye = (iota((ROWS, ROWS), 0) == iota((ROWS, ROWS), 1)).astype(F32)

    def column(row):
        return jnp.sum(eye * row, axis=1, keepdims=True)

    lane = iota((ROWS, FR), 1)
    take = []
    for j in range(2):
        sc = column(slot[j].astype(F32)).astype(jnp.int32)
        take.extend(one(lane == sc + g * CAP) for g in range(G))
    take = jnp.concatenate(take, axis=0)
    rw = rw_ref[...]
    w0, w1 = column(rw[0:1, :]), column(rw[1:2, :])
    with scope("retwait"):
        for q in range(NQ):
            remote(others(RET, q), others(B, q), rtsend.at[q], rtrecv.at[q], E, T).wait_recv()
    got = dot(take, B[...])
    for q in range(NQ):
        for g in range(G):
            a = got[g * ROWS:(g + 1) * ROWS, q * GW:(q + 1) * GW]
            b = got[(G + g) * ROWS:(G + g + 1) * ROWS, q * GW:(q + 1) * GW]
            moe_ref[:, q * QC + g * GW:q * QC + (g + 1) * GW] = (w0 * a + w1 * b).astype(BF16)

    def mix_out(q, s):
        mix_ref[:, q * QC:(q + 1) * QC] = s

    m_last(mix_out)

    with scope("drain"):
        for q in range(NQ):
            remote(others(disp, q), others(A, q), dsend.at[q], drecv.at[q], E, T).wait_send()
            remote(others(RET, q), others(B, q), rtsend.at[q], rtrecv.at[q], E, T).wait_send()
    for c in (*w_copies, h_copy):
        c.wait_send()
    key_down(sent)
    value_along(sent)
    for ys in range(NY):
        @pl.when(ys <= y_at)
        def _():
            key_along(ys, sent)
    for xs in range(NX):
        value_down(xs, sent)

    def drain_z(t, _):
        for i in range(2):
            ag_up(Z, 0, 2 * t + i).wait_send()
            ag_dn(Z, 0, 2 * t + i).wait_send()
        y_drain(t, 0)
        m_drain(t, 0)
        return 0

    lax.fori_loop(0, NZ - 1, drain_z, 0)


def make_body(cap):
    def body(mix_query, mix_key, mix_value, head_lambda, head_gain, out_weight, moe_input, moe_gain,
             expert_ids, route_weight, gate_weight, up_weight, down_weight):
        NE = lax.axis_size("ep")
        NZ = lax.axis_size("tp") // 2
        SL = mix_query.shape[0]
        ROWS, DM = moe_input.shape
        FFD = gate_weight.shape[2]
        CAP = cap if cap else 3 * ROWS * expert_ids.shape[1] // (2 * NE)
        freq = rotary_base ** (-jnp.arange(32, dtype=F32) * 2.0 / 64)
        cfg = (NE, NZ, SL, DM, FFD, ROWS, CAP)
        SLOTS, FR = NE * CAP, NE * 4 * CAP
        QC = DM // NQ
        NP = 2 * (NZ - 1)
        QT = min(512, SL)
        VM, DMA = pltpu.VMEM, pltpu.SemaphoreType.DMA
        any_ = pl.BlockSpec(memory_space=pl.ANY)
        vm = pl.BlockSpec(memory_space=pltpu.VMEM)
        sm = pl.BlockSpec(memory_space=pltpu.SMEM)
        scratch = [
            VM((ROWS, DM), BF16), VM((SL, 128), BF16), VM((SL, 128), BF16), VM((SL, 128), BF16),
            VM((2, DM, FFD), BF16), VM((2, DM, FFD), BF16), VM((2, FFD, DM), BF16), VM((2, 128, DM), BF16),
            VM((FR, QC), BF16), VM((FR, QC), BF16),
            VM((NZ, NQ, SLOTS, QC), BF16), VM((NZ, NQ, SLOTS, QC), BF16),
            VM((NP, SLOTS, QC), BF16), VM((NP, SLOTS, QC), BF16),
            VM((FR, QC), BF16), VM((FR, QC), BF16),
            VM((4 * SLOTS, FR), BF16), VM((FR, 4 * SLOTS), BF16),
            VM((NE, SL, 128), BF16), VM((NE, 128, SL), BF16), VM((128, 2 * SL), BF16),
            VM((128, 2 * SL), F32), VM((1, 2 * SL), F32), VM((1, 2 * SL), F32),
            VM((SL, QT), F32), VM((SL, QT), F32),
            VM((2, SL // 2, 128), BF16), VM((SL // 2, 128), BF16),
            VM((NZ, NQ, ROWS, QC), BF16), VM((NP, ROWS, QC), BF16), VM((NP, ROWS, QC), BF16),
            DMA((8,)), DMA((4,)), DMA((4,)), DMA((NQ,)), DMA((NQ,)), DMA((2, 2 * NE)), DMA((2, NE)),
            DMA((NP,)), DMA((NP,)), DMA((NP,)), DMA((NP,)),
            DMA((NP,)), DMA((NP,)), DMA((NP,)), DMA((NP,)),
            DMA((NQ,)), DMA((NQ,)), DMA((1,)), DMA((1,)),
            DMA((NP,)), DMA((NP,)), DMA((NP,)), DMA((NP,)),
        ]
        return pl.pallas_call(
            functools.partial(kernel, cfg),
            out_shape=(jax.ShapeDtypeStruct((ROWS, DM), BF16), jax.ShapeDtypeStruct((ROWS, DM), BF16)),
            in_specs=[any_, any_, any_, sm, vm, any_, any_, vm, vm, vm, any_, any_, any_, vm],
            out_specs=(vm, vm),
            scratch_shapes=scratch,
            compiler_params=pltpu.CompilerParams(
                collective_id=0, has_side_effects=True, vmem_limit_bytes=67043328),
            name="step",
        )(mix_query, mix_key, mix_value, head_lambda, head_gain.reshape(1, -1), out_weight, moe_input,
          moe_gain.reshape(1, -1), expert_ids.T, route_weight.T, gate_weight, up_weight, down_weight,
          freq.reshape(1, -1))

    return body


def solution(mesh, cap=None):
    return jax.shard_map(
        make_body(cap),
        mesh=mesh,
        in_specs=(
            P("ep", "tp"), P("ep", "tp"), P("ep", "tp"), P("tp"), P(), P("tp", None),
            P(("ep", "tp"), None), P(), P(("ep", "tp"), None), P(("ep", "tp"), None),
            P("ep", None, "tp"), P("ep", None, "tp"), P("ep", "tp", None),
        ),
        out_specs=(P(("ep", "tp"), None), P(("ep", "tp"), None)),
        check_vma=False,
    )
```

```python
import functools
import math

import jax
import jax.numpy as jnp
from jax import lax
from jax.experimental import pallas as pl
from jax.experimental.pallas import tpu as pltpu
from jax.sharding import PartitionSpec as P

epsilon = 1e-06
rotary_base = 10000.0
far_below = -1e30
MESH = pl.DeviceIdType.MESH
F32 = jnp.float32
BF16 = jnp.bfloat16
scope = jax.named_scope
NQ = 4
NF = 2


def remote(src, dst, send, recv, ep, tp):
    return pltpu.make_async_remote_copy(
        src_ref=src, dst_ref=dst, send_sem=send, recv_sem=recv,
        device_id={"ep": ep, "tp": tp}, device_id_type=MESH,
    )


def start(c):
    c.start()


def sent(c):
    c.wait_send()


def dot(a, b):
    return jnp.dot(a, b, preferred_element_type=F32)


def iota(shape, dim):
    return lax.broadcasted_iota(jnp.int32, shape, dim)


def one(x):
    return x.astype(F32).astype(BF16)


def kernel(cfg, *refs):
    (NE, NZ, SL, DM, FFD, ROWS, CAP) = cfg
    (q_hbm, k_hbm, v_hbm, lam_ref, gain_ref, wo_hbm, x_hbm, mgain_ref, ids_ref, rw_ref,
     wg_hbm, wu_hbm, wd_hbm, freq_ref,
     mix_ref, moe_ref,
     xin, q_in, k_in, v_in, wg, wu, wd, wo, disp, A, X, Y, RU, RD, RET, B, FY, FB, DY, DRU, DRD, info,
     KA, VT, Q2, acc, m_s, l_s, S0, S1, hb, hx, MY, MRU, MRD,
     in_sem, wsend, wrecv, dsend, drecv, kvsend, kvrecv,
     agus, agur, agds, agdr, rsus, rsur, rsds, rsdr, rtsend, rtrecv, hsend, hrecv,
     mus, mur, mds, mdr, isend, irecv, lsend, lrecv, dus, dur, dds, ddr) = refs

    E = lax.axis_index("ep")
    T = lax.axis_index("tp")
    Z = T // 2
    C = T % 2
    up_t = 2 * ((Z + 1) % NZ) + C
    dn_t = 2 * ((Z + NZ - 1) % NZ) + C
    par_t = 2 * Z + (1 - C)
    NX = math.isqrt(NE)
    NY = NE // NX
    x_at, y_at = E % NX, E // NX
    SLOTS = NE * CAP
    G = 4
    FC = G * CAP
    FR = NE * FC
    QC = DM // NQ
    GW = QC // G
    H2 = NZ // 2
    NL = NQ - NF
    SG = min(4, NE)
    GS, GF = SG * CAP, SG * FC

    def local(src, dst, i):
        return pltpu.make_async_copy(src, dst, in_sem.at[i])

    c_x = local(x_hbm, xin, 0)
    c_k = local(k_hbm, k_in, 1)
    c_v = local(v_hbm, v_in, 2)
    c_q = local(q_hbm, q_in, 3)
    c_w = [local(wg_hbm.at[0], wg.at[0], 4), local(wu_hbm.at[0], wu.at[0], 5),
           local(wd_hbm.at[0], wd.at[0], 6), local(wo_hbm, wo.at[0], 7)]
    for c in (c_x, c_k, c_v, c_q, *c_w):
        c.start()

    barrier = pltpu.get_barrier_semaphore()

    def greet(j, _):
        pl.semaphore_signal(barrier, inc=1, device_id={"ep": (E + j) % NE, "tp": T}, device_id_type=MESH)
        return 0

    lax.fori_loop(1, NE, greet, 0)

    def greet_z(j, _):
        pl.semaphore_signal(barrier, inc=1, device_id={"ep": E, "tp": (T + 2 * j) % (2 * NZ)}, device_id_type=MESH)
        return 0

    lax.fori_loop(1, NZ, greet_z, 0)
    pl.semaphore_signal(barrier, inc=1, device_id={"ep": E, "tp": par_t}, device_id_type=MESH)

    ids = ids_ref[...]
    hot = [(ids[j:j + 1, :] == iota((NE, ROWS), 0)).astype(F32) for j in range(2)]
    earlier = one(iota((ROWS, ROWS), 0) < iota((ROWS, ROWS), 1))
    before = dot((hot[0] + hot[1]).astype(BF16), earlier)
    slot = []
    for j in range(2):
        rank = jnp.sum(hot[j] * before, axis=0, keepdims=True).astype(jnp.int32)
        slot.append(ids[j:j + 1, :] * FC + rank)
    info[Z] = jnp.concatenate([slot[0].astype(F32), slot[1].astype(F32), rw_ref[...]], axis=0)
    folded = [jnp.concatenate([s + g * CAP for g in range(G)], axis=1) for s in slot]
    fr = iota((FR, G * ROWS), 0)
    send_sel = one((fr == folded[0]) | (fr == folded[1]))

    with scope("xwait"):
        c_x.wait()
    xv = xin[...].astype(F32)
    normed = (xv * lax.rsqrt(jnp.mean(xv * xv, axis=-1, keepdims=True) + epsilon) * mgain_ref[...]).astype(BF16)
    for q in range(NQ):
        part = jnp.concatenate([normed[:, q * QC + g * GW:q * QC + (g + 1) * GW] for g in range(G)], axis=0)
        disp[:, q * GW:(q + 1) * GW] = dot(send_sel, part).astype(BF16)

    def fold_of(i):
        f = i.astype(F32)
        g = jnp.floor((f + 0.5) * (1.0 / GS))
        t = f - g * GS
        return (t + jnp.floor((t + 0.5) * (1.0 / CAP)) * (FC - CAP) + g * CAP).astype(jnp.int32)

    pack = one(fold_of(iota((GF, 1), 0)) == iota((GF, GF), 1))
    unpack = one(fold_of(iota((1, GF), 1)) == iota((GF, GF), 0))

    eye32 = (iota((32, 32), 0) == iota((32, 32), 1)).astype(F32)
    freq = jnp.sum(eye32 * freq_ref[...], axis=1, keepdims=True)
    pos = (iota((32, SL), 1) + E * SL).astype(F32)
    ang = freq * pos
    cosv, sinv = jnp.cos(ang), jnp.sin(ang)

    with scope("barrier"):
        pl.semaphore_wait(barrier, NE - 1 + NZ - 1 + 1)

    def rows_of(buf, e, q):
        return buf.at[pl.ds(pl.multiple_of(e * FC, FC), FC), pl.ds(q * GW, GW)]

    def others(buf, q):
        return buf.at[pl.ds(0, (NE - 1) * FC), pl.ds(q * GW, GW)]

    for q in range(NQ):
        def send_disp(j, _):
            dst = (E + j) % NE
            remote(rows_of(disp, dst, q), rows_of(A, E, q), dsend.at[q], drecv.at[q], dst, T).start()
            return 0

        lax.fori_loop(1, NE, send_disp, 0)
    own = pl.ds(pl.multiple_of(E * FC, FC), FC)
    A[own, :] = disp[own, :]

    def info_copy(j, src):
        return remote(info.at[src], info.at[src], isend.at[j], irecv.at[src], E, (T + 2 * j) % (2 * NZ))

    def send_info(j, _):
        info_copy(j, Z).start()
        return 0

    lax.fori_loop(1, NZ, send_info, 0)

    w_copies = [
        remote(wg_hbm.at[0], wg.at[1], wsend.at[0], wrecv.at[0], E, par_t),
        remote(wu_hbm.at[0], wu.at[1], wsend.at[1], wrecv.at[1], E, par_t),
        remote(wd_hbm.at[0], wd.at[1], wsend.at[2], wrecv.at[2], E, par_t),
        remote(wo_hbm, wo.at[1], wsend.at[3], wrecv.at[3], E, par_t),
    ]
    for c in w_copies:
        c.start()

    def rotated(xt):
        parts = []
        for m in range(2):
            a = xt[64 * m:64 * m + 32, :]
            b = xt[64 * m + 32:64 * m + 64, :]
            parts.append(a * cosv - b * sinv)
            parts.append(b * cosv + a * sinv)
        return jnp.concatenate(parts, axis=0)

    with scope("kprep"):
        c_k.wait()
        kt = rotated(k_in[...].astype(F32).T)
        KA[E] = kt.T.astype(BF16)
        c_v.wait()
        VT[E] = v_in[...].T

    def pass_key(s, send, x2, y2):
        return remote(KA.at[s], KA.at[s], kvsend.at[0, send], kvrecv.at[0, s], y2 * NX + x2, T)

    def pass_value(s, send, x2, y2):
        return remote(VT.at[s], VT.at[s], kvsend.at[1, send], kvrecv.at[1, s], y2 * NX + x2, T)

    def key_down(act):
        for y2 in range(NY):
            @pl.when(y2 > y_at)
            def _():
                act(pass_key(E, NE + y2, x_at, y2))

    def key_along(ys, act):
        for x2 in range(NX):
            @pl.when((x2 != x_at) & ((ys < y_at) | (x2 > x_at)))
            def _():
                act(pass_key(ys * NX + x_at, ys * NX + x2, x2, y_at))

    def value_along(act):
        for x2 in range(NX):
            @pl.when((x2 != x_at) & ((y_at < NY - 1) | (x2 > x_at)))
            def _():
                act(pass_value(E, NE + x2, x2, y_at))

    def value_down(xs, act):
        for y2 in range(NY):
            @pl.when(y2 > y_at)
            def _():
                act(pass_value(y_at * NX + xs, y2 * NX + xs, x_at, y2))

    FWD = max(NX, NY) - 1
    P1 = NX + NY - 2

    def pass_on(f):
        ys = y_at - 1 - f

        @pl.when(ys >= 0)
        def _():
            with scope("kfwait"):
                pass_key(ys * NX + x_at, 0, x_at, y_at).wait_recv()
            key_along(ys, start)

        xs = (x_at - 1 - f + NX) % NX

        @pl.when((f < NX - 1) & ((y_at < NY - 1) | (xs < x_at)))
        def _():
            with scope("vfwait"):
                pass_value(y_at * NX + xs, 0, x_at, y_at).wait_recv()
            value_down(xs, start)

    c_q.wait()
    qt = (rotated(q_in[...].astype(F32).T) * 64 ** (-0.5)).astype(BF16)
    zero = jnp.zeros((64, SL), BF16)
    Q2[:, :SL] = jnp.concatenate([qt[:64], zero], axis=0)
    Q2[:, SL:] = jnp.concatenate([zero, qt[64:]], axis=0)
    acc[...] = jnp.zeros(acc.shape, F32)
    m_s[...] = jnp.full(m_s.shape, far_below, F32)
    l_s[...] = jnp.zeros(l_s.shape, F32)

    QT = min(512, SL)

    def diag(mp, _):
        for q0 in range(0, SL, QT):
            keys = q0 + QT
            cols = pl.ds(pl.multiple_of(mp * SL + q0, QT), QT)
            sc = dot(KA[E, :keys], Q2[:, cols])
            sc = jnp.where(iota(sc.shape, 0) <= iota(sc.shape, 1) + q0, sc, far_below)
            m_new = jnp.max(sc, axis=0, keepdims=True)
            p = jnp.exp(sc - m_new)
            m_s[:, cols] = m_new
            l_s[:, cols] = jnp.sum(p, axis=0, keepdims=True)
            acc[:, cols] = dot(VT[E, :, :keys], p.astype(BF16))
        return 0

    with scope("diag"):
        lax.fori_loop(0, 2, diag, 0)

    SB = (S0, S1)
    TILES = 2 * SL // QT

    def attend(s):
        def scores(t):
            sc = dot(KA[s], Q2[:, t * QT:(t + 1) * QT])
            SB[t % 2][...] = sc
            return jnp.max(sc, axis=0, keepdims=True)

        top = scores(0)
        for t in range(TILES):
            cols = slice(t * QT, (t + 1) * QT)
            m_old = m_s[:, cols]
            m_new = jnp.maximum(m_old, top)
            shrink = jnp.exp(m_old - m_new)
            m_s[:, cols] = m_new
            if t + 1 < TILES:
                top = scores(t + 1)
            p = jnp.exp(SB[t % 2][...] - m_new)
            l_s[:, cols] = l_s[:, cols] * shrink + jnp.sum(p, axis=0, keepdims=True)
            acc[:, cols] = acc[:, cols] * shrink + dot(VT[s], p.astype(BF16))

    def kv_block(j):
        r = j - P1
        rest = (y_at - 1 - r // max(NX - 1, 1)) * NX + (x_at - 1 - r % max(NX - 1, 1) + NX) % NX
        near = jnp.where(j < x_at, E - 1 - j, E - (j - x_at + 1) * NX)
        src = jnp.where(r < 0, near, rest)

        @pl.when(((r < 0) & (j < x_at + y_at)) | ((r >= 0) & (r < y_at * (NX - 1))))
        def _():
            with scope("kvwait"):
                @pl.when(src % NX != x_at)
                def _():
                    pass_key(src, 0, x_at, y_at).wait_recv()

                @pl.when(src // NX != y_at)
                def _():
                    pass_value(src, 0, x_at, y_at).wait_recv()

            with scope("attend"):
                attend(src)

    def ag_up(zs, q, i):
        ref = X.at[zs, q]
        return remote(ref, ref, agus.at[i], agur.at[i], E, up_t)

    def ag_dn(zs, q, i):
        ref = X.at[zs, q]
        return remote(ref, ref, agds.at[i], agdr.at[i], E, dn_t)

    for q in range(NQ):
        with scope("rowswait"):
            remote(others(disp, q), others(A, q), dsend.at[q], drecv.at[q], E, T).wait_recv()
        for n in range(NE // SG):
            rows = dot(pack, A[n * GF:(n + 1) * GF, q * GW:(q + 1) * GW])
            for g in range(G):
                X[Z, q, n * GS:(n + 1) * GS, g * GW:(g + 1) * GW] = rows[g * GS:(g + 1) * GS].astype(BF16)
        if NZ > 2 or q < 2:
            ag_up(Z, q, q).start()
        if NZ > 2 or q >= 2:
            ag_dn(Z, q, q if NZ > 2 else q - 2).start()

    key_down(start)
    value_along(start)
    key_along(y_at, start)
    value_down(x_at, start)

    with scope("wwait"):
        for c in c_w:
            c.wait()
        for c in w_copies:
            c.wait_recv()

    def fold(parts, n):
        rows = slice(n * GS, (n + 1) * GS)
        return dot(unpack, jnp.concatenate(
            [jnp.concatenate([y[rows, g * GW:(g + 1) * GW] for g in range(G)], axis=0) for y in parts], axis=1)).astype(BF16)

    def experts(zb):
        xb = jnp.concatenate([X[zb, q] for q in range(NQ)], axis=1)
        hid = []
        for w in range(2):
            g = dot(xb, wg[w])
            u = dot(xb, wu[w])
            hid.append((g / (1.0 + jnp.exp(-g)) * u).astype(BF16))
        later = []
        for q in range(NQ):
            n = slice(q * QC, (q + 1) * QC)
            y = (dot(hid[0], wd[0, :, n]) + dot(hid[1], wd[1, :, n])).astype(BF16)
            if q < NF:
                Y[zb, q] = y
            else:
                later.append(y)
        for n in range(NE // SG):
            FY[zb, n * GF:(n + 1) * GF, :] = fold(later, n)

    def make_ring(PH, buf, land_u, land_d, us, ur, ds_, dr):
        def target(t, sign):
            return (Z + sign * (H2 - (t + 1) // 2) + NZ) % NZ

        def up(t, i):
            far = 1 - jnp.minimum(t, 1)
            h = (t + 1) % 2 - far
            ref = buf.at[target(t, 1), PH * h + i]
            return ref, remote(ref, land_u.at[PH * t + i], us.at[PH * t + i], ur.at[PH * t + i], E, up_t)

        def down(t, i):
            h = (t + 1) % 2
            ref = buf.at[target(t, -1), PH * h + i]
            return ref, remote(ref, land_d.at[PH * t + i], ds_.at[PH * t + i], dr.at[PH * t + i], E, dn_t)

        def first():
            for i in range(PH):
                up(0, i)[1].start()
                down(0, i)[1].start()
            if NZ > 2:
                for i in range(PH):
                    up(2, i)[1].start()
                    down(1, i)[1].start()

        def step(s):
            for f, land, t in ((up, land_u, s + 1 - (2 - jnp.minimum(s, 2))), (down, land_d, s + 1)):
                for i in range(PH):
                    with scope("rswait"):
                        f(s - 1, i)[1].wait_recv()
                    ref, copy = f(t, i)
                    ref[...] = (ref[...].astype(F32) + land[PH * (s - 1) + i].astype(F32)).astype(BF16)
                    copy.start()

        def last(out):
            if NZ > 2:
                for h in range(2):
                    t = NZ - 3 + h
                    for i in range(PH):
                        with scope("lastwait"):
                            up(t, i)[1].wait_recv()
                            down(t, i)[1].wait_recv()
                        q = PH * h + i
                        out(q, (buf[Z, q].astype(F32) + land_u[PH * t + i].astype(F32)
                                + land_d[PH * t + i].astype(F32)).astype(BF16))
            else:
                for q in range(2 * PH):
                    f, land = (up, land_u) if q < PH else (down, land_d)
                    f(0, q % PH)[1].wait_recv()
                    out(q, (buf[Z, q].astype(F32) + land[q % PH].astype(F32)).astype(BF16))

        def drain(t, _):
            for i in range(PH):
                up(t, i)[1].wait_send()
                down(t, i)[1].wait_send()
            return 0

        return first, step, last, drain

    y_first, y_step, y_last, y_drain = make_ring(NF // 2, Y, RU, RD, rsus, rsur, rsds, rsdr)
    m_first, m_step, m_last, m_drain = make_ring(NQ // 2, MY, MRU, MRD, mus, mur, mds, mdr)

    d_first, d_step, d_last, d_drain = make_ring(NL // 2, DY, DRU, DRD, dus, dur, dds, ddr)

    def fold_rows(buf, zb, e):
        return buf.at[zb, pl.ds(pl.multiple_of(e * FC, FC), FC)]

    def fold_others(buf, zb):
        return buf.at[zb, pl.ds(0, (NE - 1) * FC)]

    def send_back(zb):
        def to(j, _):
            dst = (E + j) % NE
            remote(fold_rows(FY, zb, dst), fold_rows(FB, zb, E), lsend.at[zb], lrecv.at[zb], dst, T).start()
            return 0

        lax.fori_loop(1, NE, to, 0)
        FB[zb, own, :] = FY[zb, own, :]

    AGS = NZ - 1
    BACK = AGS - 1
    FWD0 = max(min(2, AGS - FWD), 0)
    STEPS = AGS + max(NZ - 3, 0)
    NKV = NE - 1
    counts = {12: [0, 0, 1, 1, 2, 1, 1, 2, 2, 2, 2, 1]}.get(STEPS)
    if counts is None or NE != 16:
        counts = [0] * (STEPS - 1) + [NKV]

    def after(i, n):
        return jnp.clip(i - n + 1, 0, 1)

    def block_at(i):
        return sum(c * after(i, s + 1) for s, c in enumerate(counts) if c)

    def main(i, _):
        @pl.when(i < AGS)
        def _():
            k = i // 2 + 1
            h = i % 2
            zu = (Z - k + NZ) % NZ
            zd = (Z + k) % NZ
            final = after(i, AGS - 1)
            for n in range(2):
                with scope("agwait"):
                    ag_up(zu, 2 * h + n, 2 * i + n).wait_recv()
                if NZ > 2:
                    @pl.when(i < NZ - 3)
                    def _():
                        ag_up(zu, 2 * h + n, 2 * i + n + 4).start()
            hd = h + final
            for n in range(2):
                with scope("agwait2"):
                    ag_dn(zd, 2 * hd + n, 2 * i + n).wait_recv()
                if NZ > 2:
                    @pl.when((i < NZ - 4) | (i == NZ - 3))
                    def _():
                        ag_dn(zd, 2 * hd + n, 2 * i + n + 4 - 2 * after(i, NZ - 3)).start()

            @pl.when((i >= FWD0) & (i < FWD0 + FWD))
            def _():
                pass_on(i - FWD0)

            def block(b, _):
                kb = (b + 1) // 2
                with scope("experts"):
                    experts((Z + kb * (1 - 2 * (b % 2)) + NZ) % NZ)
                return 0

            lo = i + (after(i, NZ - 2) if NZ > 2 else 0)
            hi = i + 1 + (after(i, NZ - 3) if NZ > 2 else 1)
            lax.fori_loop(lo, hi, block, 0)

        @pl.when(i == AGS - 1)
        def _():
            y_first()

        def back(b, _):
            kb = (b + 1) // 2
            send_back((Z + kb * (1 - 2 * (b % 2)) + NZ) % NZ)
            return 0

        @pl.when(i == BACK)
        def _():
            with scope("back"):
                lax.fori_loop(0, NZ, back, 0)

        if NZ > 2:
            @pl.when(i >= AGS)
            def _():
                y_step(i - AGS + 1)

        def blocks(j, _):
            kv_block(j)
            return 0

        lax.fori_loop(block_at(i), block_at(i + 1), blocks, 0)
        return 0

    lax.fori_loop(0, STEPS, main, 0)

    with scope("endloop"):
        o = acc[...] / l_s[...]
    comb = o[:, :SL] - lam_ref[0] * o[:, SL:]
    comb = comb * lax.rsqrt(jnp.mean(comb * comb, axis=0, keepdims=True) + epsilon)
    heads = (comb.T * gain_ref[...]).astype(BF16)
    for t in range(2 * NZ):
        hb[t % 2, (t // 2) * ROWS:(t // 2 + 1) * ROWS, :] = heads[t * ROWS:(t + 1) * ROWS, :]
    h_copy = remote(hb.at[1 - C], hx, hsend.at[0], hrecv.at[0], E, par_t)
    h_copy.start()

    def give_back(q, y):
        for n in range(NE // SG):
            RET[n * GF:(n + 1) * GF, q * GW:(q + 1) * GW] = fold([y], n)

        def send_ret(j, _):
            dst = (E + j) % NE
            remote(rows_of(RET, dst, q), rows_of(B, E, q), rtsend.at[q], rtrecv.at[q], dst, T).start()
            return 0

        lax.fori_loop(1, NE, send_ret, 0)

    y_last(give_back)
    B[own, :] = RET[own, :]

    eye = (iota((ROWS, ROWS), 0) == iota((ROWS, ROWS), 1)).astype(F32)
    lane = iota((ROWS, FR), 1)

    def column(row):
        return jnp.sum(eye * row, axis=1, keepdims=True)

    def tokens(zb, rows, out):
        inf = info[zb]
        sc = [column(inf[j:j + 1, :]).astype(jnp.int32) for j in range(2)]
        take = jnp.concatenate([one(lane == sc[j] + g * CAP) for j in range(2) for g in range(G)], axis=0)
        w0, w1 = column(inf[2:3, :]), column(inf[3:4, :])
        got = dot(take, rows)
        for q in range(rows.shape[1] // GW):
            for g in range(G):
                a = got[g * ROWS:(g + 1) * ROWS, q * GW:(q + 1) * GW]
                b = got[(G + g) * ROWS:(G + g + 1) * ROWS, q * GW:(q + 1) * GW]
                out(q, g, (w0 * a + w1 * b).astype(BF16))

    def dense(n, _):
        kb = (NZ - n) // 2
        zb = (Z + kb * (1 - 2 * (n % 2)) + NZ) % NZ

        @pl.when(zb != Z)
        def _():
            info_copy(0, zb).wait_recv()

        with scope("lwait"):
            remote(fold_others(FY, zb), fold_others(FB, zb), lsend.at[zb], lrecv.at[zb], E, T).wait_recv()

        def put(q, g, y):
            DY[zb, q, :, g * GW:(g + 1) * GW] = y

        with scope("dense"):
            tokens(zb, FB[zb], put)
        return 0

    with scope("hwait"):
        h_copy.wait_recv()
    for q in range(NQ):
        n = slice(q * QC, (q + 1) * QC)
        part = (dot(hb[C], wo[0, :, n]) + dot(hx[...], wo[1, :, n])).astype(BF16)
        for zd in range(NZ):
            MY[zd, q] = part[zd * ROWS:(zd + 1) * ROWS]
    with scope("mfirst"):
        m_first()
    lax.fori_loop(0, NZ, dense, 0)
    d_first()
    if NZ > 2:
        def m_loop(s, _):
            m_step(s)
            d_step(s)
            return 0

        lax.fori_loop(1, NZ - 2, m_loop, 0)

    with scope("retwait"):
        for q in range(NF):
            remote(others(RET, q), others(B, q), rtsend.at[q], rtrecv.at[q], E, T).wait_recv()

    def moe_part(q, g, y):
        moe_ref[:, q * QC + g * GW:q * QC + (g + 1) * GW] = y

    tokens(Z, B[...], moe_part)

    def mix_out(q, y):
        mix_ref[:, q * QC:(q + 1) * QC] = y

    def moe_out(q, y):
        moe_ref[:, (NF + q) * QC:(NF + q + 1) * QC] = y

    m_last(mix_out)
    d_last(moe_out)

    with scope("drain"):
        for q in range(NQ):
            remote(others(disp, q), others(A, q), dsend.at[q], drecv.at[q], E, T).wait_send()
        for q in range(NF):
            remote(others(RET, q), others(B, q), rtsend.at[q], rtrecv.at[q], E, T).wait_send()

    def drain_back(zb, _):
        remote(fold_others(FY, zb), fold_others(FB, zb), lsend.at[zb], lrecv.at[zb], E, T).wait_send()
        return 0

    lax.fori_loop(0, NZ, drain_back, 0)

    def drain_info(j, _):
        info_copy(j, Z).wait_send()
        return 0

    lax.fori_loop(1, NZ, drain_info, 0)
    for c in (*w_copies, h_copy):
        c.wait_send()
    key_down(sent)
    value_along(sent)
    for ys in range(NY):
        @pl.when(ys <= y_at)
        def _():
            key_along(ys, sent)
    for xs in range(NX):
        value_down(xs, sent)

    def drain_z(t, _):
        for i in range(2):
            ag_up(Z, 0, 2 * t + i).wait_send()
            ag_dn(Z, 0, 2 * t + i).wait_send()
        y_drain(t, 0)
        m_drain(t, 0)
        d_drain(t, 0)
        return 0

    lax.fori_loop(0, NZ - 1, drain_z, 0)


def make_body(cap):
    def body(mix_query, mix_key, mix_value, head_lambda, head_gain, out_weight, moe_input, moe_gain,
             expert_ids, route_weight, gate_weight, up_weight, down_weight):
        NE = lax.axis_size("ep")
        NZ = lax.axis_size("tp") // 2
        SL = mix_query.shape[0]
        ROWS, DM = moe_input.shape
        FFD = gate_weight.shape[2]
        CAP = cap if cap else 3 * ROWS * expert_ids.shape[1] // (2 * NE)
        freq = rotary_base ** (-jnp.arange(32, dtype=F32) * 2.0 / 64)
        cfg = (NE, NZ, SL, DM, FFD, ROWS, CAP)
        SLOTS, FR = NE * CAP, NE * 4 * CAP
        QC = DM // NQ
        NL = NQ - NF
        NP = 2 * (NZ - 1)
        QT = min(512, SL)
        VM, DMA = pltpu.VMEM, pltpu.SemaphoreType.DMA
        any_ = pl.BlockSpec(memory_space=pl.ANY)
        vm = pl.BlockSpec(memory_space=pltpu.VMEM)
        sm = pl.BlockSpec(memory_space=pltpu.SMEM)
        scratch = [
            VM((ROWS, DM), BF16), VM((SL, 128), BF16), VM((SL, 128), BF16), VM((SL, 128), BF16),
            VM((2, DM, FFD), BF16), VM((2, DM, FFD), BF16), VM((2, FFD, DM), BF16), VM((2, 128, DM), BF16),
            VM((FR, QC), BF16), VM((FR, QC), BF16),
            VM((NZ, NQ, SLOTS, QC), BF16), VM((NZ, NF, SLOTS, QC), BF16),
            VM((NZ - 1, SLOTS, QC), BF16), VM((NZ - 1, SLOTS, QC), BF16),
            VM((FR, NF * QC // 4), BF16), VM((FR, NF * QC // 4), BF16),
            VM((NZ, FR, NL * QC // 4), BF16), VM((NZ, FR, NL * QC // 4), BF16),
            VM((NZ, NL, ROWS, QC), BF16), VM((NZ - 1, ROWS, QC), BF16), VM((NZ - 1, ROWS, QC), BF16),
            VM((NZ, 4, ROWS), F32),
            VM((NE, SL, 128), BF16), VM((NE, 128, SL), BF16), VM((128, 2 * SL), BF16),
            VM((128, 2 * SL), F32), VM((1, 2 * SL), F32), VM((1, 2 * SL), F32),
            VM((SL, QT), F32), VM((SL, QT), F32),
            VM((2, SL // 2, 128), BF16), VM((SL // 2, 128), BF16),
            VM((NZ, NQ, ROWS, QC), BF16), VM((NP, ROWS, QC), BF16), VM((NP, ROWS, QC), BF16),
            DMA((8,)), DMA((4,)), DMA((4,)), DMA((NQ,)), DMA((NQ,)), DMA((2, 2 * NE)), DMA((2, NE)),
            DMA((NP,)), DMA((NP,)), DMA((NP,)), DMA((NP,)),
            DMA((NP,)), DMA((NP,)), DMA((NP,)), DMA((NP,)),
            DMA((NQ,)), DMA((NQ,)), DMA((1,)), DMA((1,)),
            DMA((NP,)), DMA((NP,)), DMA((NP,)), DMA((NP,)),
            DMA((NZ,)), DMA((NZ,)), DMA((NZ,)), DMA((NZ,)),
            DMA((NP,)), DMA((NP,)), DMA((NP,)), DMA((NP,)),
        ]
        return pl.pallas_call(
            functools.partial(kernel, cfg),
            out_shape=(jax.ShapeDtypeStruct((ROWS, DM), BF16), jax.ShapeDtypeStruct((ROWS, DM), BF16)),
            in_specs=[any_, any_, any_, sm, vm, any_, any_, vm, vm, vm, any_, any_, any_, vm],
            out_specs=(vm, vm),
            scratch_shapes=scratch,
            compiler_params=pltpu.CompilerParams(
                collective_id=0, has_side_effects=True, vmem_limit_bytes=67043328),
            name="step",
        )(mix_query, mix_key, mix_value, head_lambda, head_gain.reshape(1, -1), out_weight, moe_input,
          moe_gain.reshape(1, -1), expert_ids.T, route_weight.T, gate_weight, up_weight, down_weight,
          freq.reshape(1, -1))

    return body


def solution(mesh, cap=None):
    return jax.shard_map(
        make_body(cap),
        mesh=mesh,
        in_specs=(
            P("ep", "tp"), P("ep", "tp"), P("ep", "tp"), P("tp"), P(), P("tp", None),
            P(("ep", "tp"), None), P(), P(("ep", "tp"), None), P(("ep", "tp"), None),
            P("ep", None, "tp"), P("ep", None, "tp"), P("ep", "tp", None),
        ),
        out_specs=(P(("ep", "tp"), None), P(("ep", "tp"), None)),
        check_vma=False,
    )
```
